32 devices in a mesh: rep: 4 (over z), fs: 4 (over y, x), tp: 2 (over core).
Axes of the slice: x: 2, y: 2, z: 4, core: 2. Of those that a mesh axis runs over, the one named last changes fastest.
Arguments:
- tokens_in: bfloat16 [8192, 2048], P(('rep', 'fs', 'tp')), may hold values from -6 to 6
- norm_gain: float32 [2048], replicated, may hold values from 0.1 to 1.9
- gate_weight: bfloat16 [2048, 3072], P(None, ('fs', 'tp')), may hold values from -0.125 to 0.125
- up_weight: bfloat16 [2048, 3072], P(None, ('fs', 'tp')), may hold values from -0.125 to 0.125
- down_weight: bfloat16 [3072, 2048], P(('fs', 'tp')), may hold values from -0.109375 to 0.109375
- out_grad: bfloat16 [8192, 2048], P(('rep', 'fs', 'tp')), may hold values from -6 to 6
Outputs:
- grad_in: bfloat16 [8192, 2048], P(('rep', 'fs', 'tp'))
- grad_gain: float32 [2048], replicated
- grad_gate: float32 [2048, 3072], P(None, ('fs', 'tp'))
- grad_up: float32 [2048, 3072], P(None, ('fs', 'tp'))
- grad_down: float32 [3072, 2048], P(('fs', 'tp'))
The draws below stay inside these ranges and needn't reach their ends.
All inputs are finite; a program needn't handle non-finite values.
Results may differ from the reference program's by a relative error of at most 0.014.
Values may be sent and summed in bfloat16 or wider, within the bound.
A program may use at most 192 MiB of HBM per device.

```python
import jax
import jax.numpy as jnp
from jax import lax

D = 2048
FF = 3072
TOKENS = 8192
BLOCKS = 8


def strengthened(entries, key, source, target, shards_of, factor):
    def block_of(axis_at):
        return (jnp.arange(entries.shape[axis_at]) // (entries.shape[axis_at] // shards_of)).reshape((-1,) + (1,) * (entries.ndim - 1 - axis_at))

    first = jax.random.permutation(key, shards_of)[block_of(target)]
    far = (block_of(target) + shards_of // 2) % shards_of
    return jnp.where((block_of(source) == first) | (block_of(source) == far), factor * entries, entries)


def shard_levels(rng, dims, split, smallest, high):
    factor_of, own = 1.0, jax.random.fold_in(rng, 6)
    for axis_at, shards_of in split:
        draws = jnp.exp(jax.random.uniform(jax.random.fold_in(own, axis_at), (shards_of,), jnp.float32, smallest / len(split), high / len(split)))
        factor_of = factor_of * jnp.repeat(draws, dims[axis_at] // shards_of).reshape([-1 if axis == axis_at else 1 for axis in range(len(dims))])
    return factor_of


def normal_values(rng, extent, scale, most, cuts=(), held_as=jnp.bfloat16):
    drawn = jax.random.normal(rng, extent, jnp.float32) * scale
    if len(cuts) > 0:
        drawn = shard_levels(rng, extent, cuts, -0.22, 0.18) * drawn
    return jnp.clip(drawn, min=-most, max=most).astype(held_as)


def noise_with(key, dims, scale, reach, shards, heavy, dtype=jnp.bfloat16):
    array = scale * jax.random.normal(key, dims, jnp.float32)
    if shards:
        array = array * shard_levels(key, dims, shards, -0.22, 0.18)
    return jnp.clip(strengthened(array, jax.random.fold_in(key, 3), *heavy), -reach, reach).astype(dtype)


def setup_inputs(seed: int = 0) -> dict:
    key_of = jax.random.split(jax.random.key(seed), 7)
    return {
        "tokens_in": normal_values(key_of[0], (TOKENS, D), 1.0, 6.0, ((0, 32),)),
        "norm_gain": jnp.clip(1.0 + 0.18 * jax.random.normal(key_of[1], (D,), jnp.float32), 0.1, 1.9),
        "gate_weight": normal_values(key_of[2], (D, FF), D ** -0.5, 0.125, ((1, 8),)),
        "up_weight": normal_values(key_of[3], (D, FF), D ** -0.5, 0.125, ((1, 8),)),
        "down_weight": normal_values(key_of[4], (FF, D), FF ** -0.5, 0.109375, ((0, 8),)),
        "out_grad": noise_with(key_of[5], (TOKENS, D), 1.0, 6.0, ((0, 32),), (0, 1, 32, 2.75)),
    }


norm_eps = 1e-06

def reference(tokens_in, norm_gain, gate_weight, up_weight, down_weight, out_grad):
    floats = tokens_in.astype(jnp.float32)
    inverse = lax.rsqrt(lax.optimization_barrier(jnp.mean(floats * floats, axis=-1, keepdims=True)) + norm_eps)
    unit_rows = floats * inverse
    normed = (unit_rows * norm_gain).astype(jnp.bfloat16)
    gate_pre = jnp.dot(normed, gate_weight, preferred_element_type=jnp.float32)
    up_pre = jnp.dot(normed, up_weight, preferred_element_type=jnp.float32)
    sigma = jax.nn.sigmoid(gate_pre)
    active = gate_pre * sigma
    hidden = (active * up_pre).astype(jnp.bfloat16)
    grad_hidden = 0.5 * jnp.dot(out_grad, down_weight.T, preferred_element_type=jnp.float32)
    grad_gate_pre = (grad_hidden * up_pre * sigma * (1.0 + gate_pre * (1.0 - sigma))).astype(jnp.bfloat16)
    grad_up_pre = (grad_hidden * active).astype(jnp.bfloat16)
    factor = float(TOKENS) ** (-0.5)
    grad_down = jnp.dot(hidden.T, out_grad, preferred_element_type=jnp.float32) * (0.5 * factor)
    grad_gate = jnp.dot(normed.T, grad_gate_pre, preferred_element_type=jnp.float32) * factor
    grad_up = jnp.dot(normed.T, grad_up_pre, preferred_element_type=jnp.float32) * factor
    width = FF // BLOCKS
    grad_normed = jnp.zeros(floats.shape, jnp.float32)
    for block in range(BLOCKS):
        lower = block * width
        term = jnp.dot(grad_gate_pre[:, lower:lower + width], gate_weight[:, lower:lower + width].T, preferred_element_type=jnp.float32)
        term = term + jnp.dot(grad_up_pre[:, lower:lower + width], up_weight[:, lower:lower + width].T, preferred_element_type=jnp.float32)
        grad_normed = grad_normed + term.astype(jnp.bfloat16).astype(jnp.float32)
    grad_gain = lax.optimization_barrier(jnp.sum(grad_normed * unit_rows, axis=0))
    scaled = grad_normed * norm_gain
    grad_in = out_grad.astype(jnp.float32) + inverse * scaled - unit_rows * inverse * lax.optimization_barrier(jnp.mean(scaled * unit_rows, axis=-1, keepdims=True))
    return (grad_in.astype(jnp.bfloat16), grad_gain, grad_gate, grad_up, grad_down)
```

```python
import jax
import jax.numpy as jnp
from jax import lax
from jax.experimental import pallas as pl
from jax.experimental.pallas import tpu as pltpu
from jax.sharding import PartitionSpec as P

norm_eps = 1e-06
MESH = pl.DeviceIdType.MESH
F32, BF16 = jnp.float32, jnp.bfloat16
NT = (((1,), (1,)), ((), ()))
PARTS = 8
AHEAD = 2
SUB = 2
LAG_IN = 1
LAG_FIN = 3
LAG_OUT = 5
EXIT_TICK = 2 * PARTS + 2
FINISH = 30


def flip(f, j):
    return (f % 2 + j % 2) % 2 + 2 * ((f // 2 + j // 2) % 2)


def remote(src, dst, send, recv, dev):
    return pltpu.make_async_remote_copy(
        src_ref=src, dst_ref=dst, send_sem=send, recv_sem=recv, device_id=dev, device_id_type=MESH
    )


def fused_kernel(
    reps, factor,
    x_hbm, g_hbm, gain_ref, gw_hbm, uw_hbm, dw_hbm,
    gi_out, gg_out, down_out, gate_out, up_out,
    nall, gall, wcat, dwc, act, gh, tcat, gcat, own, inc, fin,
    tbuf, pin, rsin, xbuf, stage_d, stage_g, gv, gr, grep,
    ssem, rsem, lsem, up_send, in_recv, down_send, fin_recv,
    p_send, p_recv, s_send, s_recv, v_send, v_recv, w_send, w_recv, osem,
):
    f, t, r = lax.axis_index("fs"), lax.axis_index("tp"), lax.axis_index("rep")
    other = 1 - t
    parts, rk, d = xbuf.shape
    rows = parts * rk
    ff = dwc.shape[1]
    cw = d // parts
    ranks = gcat.shape[1]
    toks = ranks * rk
    chunks = 3 * parts
    sub = ff // SUB

    middle = reps // 2
    sign = 1 - 2 * (r // middle)
    up, down = {"rep": r + sign}, {"rep": (r - sign + reps) % reps}
    right = r // middle
    depth = (1 - right) * (middle - 1 - r) + right * (r - middle)
    center, outer = depth == 0, depth == middle - 1
    inner, has_down = depth > 0, depth < middle - 1
    to_a, to_b, to_p = {"fs": flip(f, 1)}, {"fs": flip(f, 2)}, {"tp": other}

    barrier = pltpu.get_barrier_semaphore()
    for dev in (to_a, to_b, {"fs": flip(f, 3)}, to_p):
        pl.semaphore_signal(barrier, inc=1, device_id=dev, device_id_type=MESH)
    for i in range(1, reps):
        pl.semaphore_signal(barrier, inc=1, device_id={"rep": (r + i) % reps}, device_id_type=MESH)

    def pos(j, core):
        return flip(f, j) * 2 + core

    me = pos(0, t)

    def loads():
        out = [pltpu.make_async_copy(x_hbm, xbuf, lsem.at[0])]
        out.append(pltpu.make_async_copy(gw_hbm, wcat.at[:, pl.ds(0, ff)], lsem.at[1]))
        out.append(pltpu.make_async_copy(uw_hbm, wcat.at[:, pl.ds(ff, ff)], lsem.at[2]))
        for c in range(parts):
            cols = pl.ds(c * cw, cw)
            out.append(pltpu.make_async_copy(g_hbm.at[:, :, cols], gall.at[c, :, me], lsem.at[3 + c]))
        for c in range(parts):
            cols = pl.ds(c * cw, cw)
            out.append(pltpu.make_async_copy(dw_hbm.at[:, cols], dwc.at[c], lsem.at[3 + parts + c]))
        return out

    local = loads()
    for c in local:
        c.start()

    def slot(ph, k, p, part=0):
        if ph == 0:
            ref = nall.at[k, p]
            size = rk // 2
        else:
            ref = gall.at[k, :, p]
            size = parts // 2
        if part == 0:
            return ref
        return ref.at[pl.ds((part - 1) * size, size)]

    def copy(ph, k, kind, incoming=False):
        sems = (ssem.at[kind, ph * parts + k], rsem.at[kind, ph * parts + k])
        core = other if incoming else t
        if kind == 0:
            ref, dev = slot(ph, k, pos(1, t) if incoming else me), to_a
        elif kind == 1:
            ref, dev = slot(ph, k, pos(2, t) if incoming else me), to_b
        elif kind == 2:
            ref, dev = slot(ph, k, pos(0, core)), to_p
        elif kind == 3:
            ref, dev = slot(ph, k, pos(3, t) if incoming else pos(1, t), 2), to_b
        elif kind == 4:
            ref, dev = slot(ph, k, pos(3, t) if incoming else pos(2, t), 1), to_a
        elif kind == 5:
            ref, dev = slot(ph, k, pos(1, core)), to_p
        elif kind == 6:
            ref, dev = slot(ph, k, pos(2, core)), to_p
        else:
            ref, dev = slot(ph, k, pos(3, core), kind - 6), to_p
        return remote(ref, ref, *sems, dev)

    def normalise(k):
        floats = xbuf[k].astype(F32)
        inverse = lax.rsqrt(jnp.mean(floats * floats, axis=-1, keepdims=True) + norm_eps)
        nall[k, me] = (floats * inverse * gain_ref[...]).astype(BF16)

    def issue(ph, k):
        if ph == 0:
            normalise(k)
        for kind in (0, 1, 2):
            copy(ph, k, kind).start()

    local[0].wait()
    pl.semaphore_wait(barrier, 3 + reps)
    for k in range(AHEAD):
        issue(0, k)
    for c in local[3:3 + parts]:
        c.wait()

    def forward(k):
        block = nall[k].reshape(toks, d)
        pre = jnp.dot(block, wcat[...], preferred_element_type=F32)
        gate_pre, up_pre = pre[:, :ff], pre[:, ff:]
        sigma = jax.nn.sigmoid(gate_pre)
        active = gate_pre * sigma
        act[k, :, pl.ds(0, ff)] = up_pre * sigma * (1.0 + gate_pre * (1.0 - sigma))
        act[k, :, pl.ds(ff, ff)] = active
        cols = pl.ds(pl.multiple_of(k * toks, toks), toks)
        tcat[pl.ds(0, ff), cols] = (active * up_pre).T.astype(BF16)

    def grad_chunk(c):
        whole = gall[c].reshape(parts * toks, cw)
        own[c] = jnp.dot(tcat[pl.ds(0, ff), :], whole, preferred_element_type=F32).astype(BF16)

        def one(k, carry):
            block = gall[c, k].reshape(toks, cw)
            part = lax.dot_general(block, dwc[c], NT, preferred_element_type=F32)

            @pl.when(c == 0)
            def _():
                gh[k] = part

            @pl.when(c > 0)
            def _():
                gh[k] = gh[k] + part

            return carry

        lax.fori_loop(0, parts, one, 0)

    def elementwise(k, carry):
        half = 0.5 * gh[k]
        ggp = half * act[k, :, pl.ds(0, ff)]
        gup = half * act[k, :, pl.ds(ff, ff)]
        cols = pl.ds(pl.multiple_of(k * toks, toks), toks)
        gcat[k, :, :, pl.ds(0, ff)] = ggp.astype(BF16).reshape(ranks, rk, ff)
        gcat[k, :, :, pl.ds(ff, ff)] = gup.astype(BF16).reshape(ranks, rk, ff)
        tcat[pl.ds(0, ff), cols] = ggp.T.astype(BF16)
        tcat[pl.ds(ff, ff), cols] = gup.T.astype(BF16)
        return carry

    def weight_chunk(s):
        a, c = s // parts - 1, s % parts
        left = tcat[pl.ds(pl.multiple_of(a * ff, ff), ff), :]
        cols = pl.ds(pl.multiple_of(c * cw, cw), cw)
        whole = nall[:, :, :, cols].reshape(parts * toks, cw)
        own[s] = jnp.dot(left, whole, preferred_element_type=F32).astype(BF16)

    def piece(ref, s, h):
        return ref.at[s, pl.ds(h * sub, sub)]

    def up_copy(s, h, src, dst, recv):
        return remote(piece(src, s, h), piece(dst, s, h), up_send.at[s, h], recv.at[s, h], up)

    def down_copy(s, h):
        return remote(piece(fin, s, h), piece(fin, s, h), down_send.at[s, h], fin_recv.at[s, h], down)

    def down_store(s):
        cols = pl.ds(pl.multiple_of(s * cw, cw), cw)
        return pltpu.make_async_copy(stage_d.at[s % 2], down_out.at[:, cols], osem.at[s % 2])

    def gate_store(s, out):
        here = pl.ds(pl.multiple_of((s % parts) * cw, cw), cw)
        return pltpu.make_async_copy(stage_g.at[s % 2], out.at[here], osem.at[2 + s % 2])

    def emit(s):
        @pl.when(s < parts)
        def _():
            @pl.when(s >= 2)
            def _():
                down_store(s - 2).wait()

            stage_d[s % 2] = fin[s].astype(F32) * (0.5 * factor)
            down_store(s).start()

        @pl.when(s >= parts)
        def _():
            @pl.when(s >= parts + 2)
            def _():
                gate_store(s - 2, gate_out).wait()

            stage_g[s % 2] = (fin[s].astype(F32) * factor).T

            @pl.when(s < 2 * parts)
            def _():
                gate_store(s, gate_out).start()

            @pl.when(s >= 2 * parts)
            def _():
                gate_store(s, up_out).start()

    def reduce_step(z):
        @pl.when(outer & (z >= 0) & (z < chunks))
        def _():
            for h in range(SUB):
                @pl.when(center)
                def _():
                    up_copy(z, h, own, fin, fin_recv).start()

                @pl.when(inner)
                def _():
                    up_copy(z, h, own, inc, in_recv).start()

        s_in = z - LAG_IN

        @pl.when(has_down & (s_in >= 0) & (s_in < chunks))
        def _():
            for h in range(SUB):
                up_copy(s_in, h, inc, inc, in_recv).wait_recv()
                here = piece(inc, s_in, h)
                here[...] = (piece(own, s_in, h)[...].astype(F32) + here[...].astype(F32)).astype(BF16)

                @pl.when(center)
                def _():
                    up_copy(s_in, h, inc, fin, fin_recv).start()

                @pl.when(inner)
                def _():
                    up_copy(s_in, h, inc, inc, in_recv).start()

        s_fin = z - jnp.where(center, LAG_FIN, LAG_OUT)

        @pl.when((s_fin >= 0) & (s_fin < chunks))
        def _():
            for h in range(SUB):
                down_copy(s_fin, h).wait_recv()
                here = piece(fin, s_fin, h)

                @pl.when(center & has_down)
                def _():
                    here[...] = (piece(inc, s_fin, h)[...].astype(F32) + here[...].astype(F32)).astype(BF16)

                @pl.when(center & outer)
                def _():
                    here[...] = (piece(own, s_fin, h)[...].astype(F32) + here[...].astype(F32)).astype(BF16)

                @pl.when(has_down)
                def _():
                    down_copy(s_fin, h).start()

            emit(s_fin)

    def pair_copy(j):
        return remote(tbuf.at[(3 - j) % 2], pin.at[j], p_send.at[j], p_recv.at[j], to_p)

    def peer_copy(j):
        return remote(pin.at[j], rsin.at[j - 1], s_send.at[j], s_recv.at[j], {"fs": flip(f, j)})

    def term(owner, c):
        cols = pl.ds(pl.multiple_of(c * cw, cw), cw)
        block = gcat[:, owner].reshape(rows, 2 * ff)
        return lax.dot_general(block, wcat[cols, :], NT, preferred_element_type=F32).astype(BF16), cols

    def exit_step(i):
        @pl.when((i >= 0) & (i < 4))
        def _():
            j = 3 - i

            @pl.when(i >= 2)
            def _():
                pair_copy(j + 2).wait_send()

            def one(c, carry):
                value, cols = term(flip(f, j) * 2 + other, c)
                tbuf[i % 2, :, cols] = value
                return carry

            lax.fori_loop(0, parts, one, 0)
            pair_copy(j).start()

        @pl.when((i >= 1) & (i < 5))
        def _():
            j = 4 - i
            pair_copy(j).wait_recv()

            def one(c, carry):
                value, cols = term(flip(f, j) * 2 + t, c)
                total = value.astype(F32) + pin[j, :, cols].astype(F32)
                gh[c, :, pl.ds(0, cw)] = total
                pin[j, :, cols] = total.astype(BF16)
                return carry

            lax.fori_loop(0, parts, one, 0)

            @pl.when(j > 0)
            def _():
                peer_copy(j).start()

    def vec_copy(n):
        dev = (to_p, to_a, to_b)[n]
        return remote(gv.at[n], gr.at[n], v_send.at[n], v_recv.at[n], dev)

    def rep_copy(i, incoming=False):
        at = (r - i + reps) % reps if incoming else r
        return remote(grep.at[at], grep.at[at], w_send.at[i], w_recv.at[i], {"rep": (r + i) % reps})

    def finish():
        for j in (3, 2, 1):
            peer_copy(j).wait_recv()
        gv[0] = jnp.zeros_like(gv[0])

        def one(k, carry):
            here = pl.ds(pl.multiple_of(k * rk, rk), rk)
            grads = jnp.concatenate([gh[c, here, pl.ds(0, cw)] for c in range(parts)], axis=1)
            for j in (2, 1, 0):
                grads = grads + rsin[j, here, :].astype(F32)
            floats = xbuf[k].astype(F32)
            inverse = lax.rsqrt(jnp.mean(floats * floats, axis=-1, keepdims=True) + norm_eps)
            unit = floats * inverse
            gv[0] = gv[0] + jnp.sum(grads * unit, axis=0, keepdims=True)
            scaled = grads * gain_ref[...]
            shift = inverse * jnp.mean(scaled * unit, axis=-1, keepdims=True)
            cot = jnp.concatenate([gall[c, k, me] for c in range(parts)], axis=1).astype(F32)
            xbuf[k] = (cot + inverse * scaled - unit * shift).astype(BF16)
            return carry

        lax.fori_loop(0, parts, one, 0)
        pltpu.make_async_copy(xbuf, gi_out, lsem.at[0]).start()
        vec_copy(0).start()

    def tick(q, carry):
        for ph in (0, 1):
            k = q - ph * parts

            @pl.when((k >= 0) & (k < parts))
            def _():
                copy(ph, k, 0, True).wait_recv()
                copy(ph, k, 3).start()
                copy(ph, k, 5).start()
                copy(ph, k, 1, True).wait_recv()
                copy(ph, k, 4).start()
                copy(ph, k, 6).start()

        for ph in (0, 1):
            k = q + AHEAD - ph * parts

            @pl.when((k >= 0) & (k < parts))
            def _():
                issue(ph, k)

        @pl.when(q == 2)
        def _():
            for c in local[1:3]:
                c.wait()

        @pl.when(q == parts + 2)
        def _():
            for c in local[3 + parts:]:
                c.wait()

        for ph in (0, 1):
            k = q - 2 - ph * parts

            @pl.when((k >= 0) & (k < parts))
            def _():
                for kind in (2, 5, 6, 7, 8):
                    copy(ph, k, kind, True).wait_recv()
                if ph == 0:
                    forward(k)
                else:
                    grad_chunk(k)

        z = q - parts - 2

        @pl.when((z >= parts) & (z < chunks))
        def _():
            weight_chunk(z)

        reduce_step(z)

        for ph in (0, 1):
            k = q - 1 - ph * parts

            @pl.when((k >= 0) & (k < parts))
            def _():
                copy(ph, k, 3, True).wait_recv()
                copy(ph, k, 8).start()
                copy(ph, k, 4, True).wait_recv()
                copy(ph, k, 7).start()

        @pl.when(q == EXIT_TICK - 1)
        def _():
            lax.fori_loop(0, parts, elementwise, 0)

        exit_step(q - EXIT_TICK)

        @pl.when(q == FINISH)
        def _():
            finish()

        for n in (0, 1, 2):
            @pl.when(q == FINISH + 1 + n)
            def _():
                vec_copy(n).wait_recv()
                gv[n + 1] = gv[n] + gr[n]
                if n < 2:
                    vec_copy(n + 1).start()
                else:
                    grep[r] = gv[3]
                    for i in range(1, reps):
                        rep_copy(i).start()

        return carry

    ticks = parts + 2 + chunks + LAG_OUT
    lax.fori_loop(0, ticks, tick, 0)

    for i in range(1, reps):
        rep_copy(i, True).wait_recv()
    total = grep[0]
    for i in range(1, reps):
        total = total + grep[i]
    for n in range(3):
        vec_copy(n).wait_send()
    gv[0] = total
    last = pltpu.make_async_copy(gv.at[0], gg_out, lsem.at[1])
    last.start()

    def drain(k, carry):
        for ph in (0, 1):
            for kind in range(9):
                copy(ph, k, kind).wait_send()
        return carry

    lax.fori_loop(0, parts, drain, 0)

    def drain_reduce(s, carry):
        for h in range(SUB):
            up_copy(s, h, own, inc, in_recv).wait_send()

            @pl.when(has_down)
            def _():
                down_copy(s, h).wait_send()

        return carry

    lax.fori_loop(0, chunks, drain_reduce, 0)
    for j in (1, 0):
        pair_copy(j).wait_send()
    for j in (3, 2, 1):
        peer_copy(j).wait_send()
    for i in range(1, reps):
        rep_copy(i).wait_send()
    for s in (parts - 2, parts - 1):
        down_store(s).wait()
    for s in (chunks - 2, chunks - 1):
        gate_store(s, up_out).wait()
    pltpu.make_async_copy(xbuf, gi_out, lsem.at[0]).wait()
    last.wait()


def shards(tokens_in, norm_gain, gate_weight, up_weight, down_weight, out_grad):
    rows, d = tokens_in.shape
    ff = gate_weight.shape[1]
    reps = lax.axis_size("rep")
    ranks = lax.axis_size("fs") * lax.axis_size("tp")
    factor = float(rows * reps * ranks) ** (-0.5)
    rk, cw = rows // PARTS, d // PARTS
    vmem, anywhere = pl.BlockSpec(memory_space=pltpu.VMEM), pl.BlockSpec(memory_space=pl.ANY)
    dma = pltpu.SemaphoreType.DMA
    chunks = 3 * PARTS
    shape = lambda *s: jax.ShapeDtypeStruct(s, F32)
    narrow = lambda *s: pltpu.VMEM(s, BF16)
    wide = lambda *s: pltpu.VMEM(s, F32)
    grad_in, grad_gain, grad_down, grad_gate, grad_up = pl.pallas_call(
        lambda *refs: fused_kernel(reps, factor, *refs),
        out_shape=[
            jax.ShapeDtypeStruct((PARTS, rk, d), BF16), shape(1, d), shape(ff, d), shape(d, ff), shape(d, ff),
        ],
        in_specs=[anywhere, anywhere, vmem, anywhere, anywhere, anywhere],
        out_specs=[anywhere] * 5,
        scratch_shapes=[
            narrow(PARTS, ranks, rk, d), narrow(PARTS, PARTS, ranks, rk, cw),
            narrow(d, 2 * ff), narrow(PARTS, ff, cw),
            wide(PARTS, ranks * rk, 2 * ff), wide(PARTS, ranks * rk, ff),
            narrow(2 * ff, PARTS * ranks * rk), narrow(PARTS, ranks, rk, 2 * ff),
            narrow(chunks, ff, cw), narrow(chunks, ff, cw), narrow(chunks, ff, cw),
            narrow(2, rows, d), narrow(4, rows, d), narrow(3, rows, d), narrow(PARTS, rk, d),
            wide(2, ff, cw), wide(2, cw, ff), wide(4, 1, d), wide(3, 1, d), wide(reps, 1, d),
            dma((9, 2 * PARTS)), dma((9, 2 * PARTS)), dma((3 + 2 * PARTS,)),
            dma((chunks, SUB)), dma((chunks, SUB)), dma((chunks, SUB)), dma((chunks, SUB)),
            dma((4,)), dma((4,)), dma((4,)), dma((4,)), dma((3,)), dma((3,)), dma((reps,)), dma((reps,)), dma((4,)),
        ],
        compiler_params=pltpu.CompilerParams(
            collective_id=0, has_side_effects=True, vmem_limit_bytes=63 * 2**20
        ),
        name="fused_backward",
    )(
        tokens_in.reshape(PARTS, rk, d), out_grad.reshape(PARTS, rk, d), norm_gain.reshape(1, d),
        gate_weight, up_weight, down_weight,
    )
    return (grad_in.reshape(rows, d), grad_gain.reshape(d), grad_gate, grad_up, grad_down)


def solution(mesh):
    spread = ("fs", "tp")
    in_specs = (
        P(("rep", "fs", "tp"), None), P(), P(None, spread), P(None, spread), P(spread, None),
        P(("rep", "fs", "tp"), None),
    )
    out_specs = (
        P(("rep", "fs", "tp"), None), P(), P(None, spread), P(None, spread), P(spread, None),
    )
    return jax.shard_map(shards, mesh=mesh, in_specs=in_specs, out_specs=out_specs, check_vma=False)
```

```python
import jax
import jax.numpy as jnp
from jax import lax
from jax.experimental import pallas as pl
from jax.experimental.pallas import tpu as pltpu
from jax.sharding import PartitionSpec as P

norm_eps = 1e-06
MESH = pl.DeviceIdType.MESH
F32, BF16 = jnp.float32, jnp.bfloat16
NT = (((1,), (1,)), ((), ()))
PARTS = 8
AHEAD = 2
PIECES = 4
SUB = 2
LAG_IN = 1
LAG_FIN = 3
LAG_OUT = 6
EXIT_TICK = 2 * PARTS + 2
UNROLL = 4
LAG_SEND = 4
FINISH = 31


def flip(f, j):
    return (f % 2 + j % 2) % 2 + 2 * ((f // 2 + j // 2) % 2)


def remote(src, dst, send, recv, dev):
    return pltpu.make_async_remote_copy(
        src_ref=src, dst_ref=dst, send_sem=send, recv_sem=recv, device_id=dev, device_id_type=MESH
    )


def fused_kernel(
    reps,
    x_hbm, g_hbm, gain_ref, gw_hbm, uw_hbm, dw_hbm,
    gi_out, gg_out, down_out, gate_out, up_out,
    nall, gall, wcat, dwt, act, gh, tcat, gcat, own, inc, fin,
    tbuf, pin, rsin, xbuf, stage_g, gv, gr, grep,
    ssem, rsem, lsem, up_send, in_recv, down_send, fin_recv,
    p_send, p_recv, s_send, s_recv, v_send, v_recv, w_send, w_recv, osem,
):
    f, t, r = lax.axis_index("fs"), lax.axis_index("tp"), lax.axis_index("rep")
    other = 1 - t
    parts, rk, d = xbuf.shape
    rows = parts * rk
    ff = dwt.shape[2]
    cw = d // parts
    ranks = gcat.shape[1]
    toks = ranks * rk
    chunks = 3 * parts
    sub = ff // SUB
    turn = 2 * ff // toks

    middle = reps // 2
    sign = 1 - 2 * (r // middle)
    up, down = {"rep": r + sign}, {"rep": (r - sign + reps) % reps}
    right = r // middle
    depth = (1 - right) * (middle - 1 - r) + right * (r - middle)
    center, outer = depth == 0, depth == middle - 1
    inner, has_down = depth > 0, depth < middle - 1
    to_a, to_b, to_p = {"fs": flip(f, 1)}, {"fs": flip(f, 2)}, {"tp": other}

    barrier = pltpu.get_barrier_semaphore()
    for dev in (to_a, to_b, {"fs": flip(f, 3)}, to_p):
        pl.semaphore_signal(barrier, inc=1, device_id=dev, device_id_type=MESH)
    for i in range(1, reps):
        pl.semaphore_signal(barrier, inc=1, device_id={"rep": (r + i) % reps}, device_id_type=MESH)

    def pos(j, core):
        return flip(f, j) * 2 + core

    me = pos(0, t)

    def loads():
        out = [pltpu.make_async_copy(x_hbm, xbuf, lsem.at[0])]
        out.append(pltpu.make_async_copy(gw_hbm, wcat.at[:, pl.ds(0, ff)], lsem.at[1]))
        out.append(pltpu.make_async_copy(uw_hbm, wcat.at[:, pl.ds(ff, ff)], lsem.at[2]))
        for c in range(parts):
            cols = pl.ds(c * cw, cw)
            out.append(pltpu.make_async_copy(g_hbm.at[:, :, cols], gall.at[c, :, me], lsem.at[3 + c]))
        for c in range(parts):
            cols = pl.ds(c * cw, cw)
            out.append(pltpu.make_async_copy(dw_hbm.at[:, cols], own.at[2 * parts + c], lsem.at[3 + parts + c]))
        return out

    local = loads()
    for c in local:
        c.start()

    def slot(ph, k, p, part=0):
        if ph == 0:
            ref = nall.at[k, p]
            size = rk // 2
        else:
            ref = gall.at[k, :, p]
            size = parts // 2
        if part == 0:
            return ref
        return ref.at[pl.ds((part - 1) * size, size)]

    def copy(ph, k, kind, incoming=False):
        sems = (ssem.at[kind, ph * parts + k], rsem.at[kind, ph * parts + k])
        core = other if incoming else t
        if kind == 0:
            ref, dev = slot(ph, k, pos(1, t) if incoming else me), to_a
        elif kind == 1:
            ref, dev = slot(ph, k, pos(2, t) if incoming else me), to_b
        elif kind == 2:
            ref, dev = slot(ph, k, pos(0, core)), to_p
        elif kind == 3:
            ref, dev = slot(ph, k, pos(3, t) if incoming else pos(1, t), 2), to_b
        elif kind == 4:
            ref, dev = slot(ph, k, pos(3, t) if incoming else pos(2, t), 1), to_a
        elif kind == 5:
            ref, dev = slot(ph, k, pos(1, core)), to_p
        elif kind == 6:
            ref, dev = slot(ph, k, pos(2, core)), to_p
        else:
            ref, dev = slot(ph, k, pos(3, core), kind - 6), to_p
        return remote(ref, ref, *sems, dev)

    def normalise(k):
        floats = xbuf[k].astype(F32)
        inverse = lax.rsqrt(jnp.mean(floats * floats, axis=-1, keepdims=True) + norm_eps)
        nall[k, me] = (floats * inverse * gain_ref[...]).astype(BF16)

    def issue(ph, k):
        for kind in (0, 1, 2):
            copy(ph, k, kind).start()

    local[0].wait()
    for k in range(AHEAD):
        normalise(k)
    pl.semaphore_wait(barrier, 3 + reps)
    for k in range(AHEAD):
        issue(0, k)
    for c in local[3:3 + parts]:
        c.wait()

    def forward(k):
        block = nall[k].reshape(toks, d)
        pre = jnp.dot(block, wcat[...], preferred_element_type=F32)
        gate_pre, up_pre = pre[:, :ff], pre[:, ff:]
        sigma = jax.nn.sigmoid(gate_pre)
        active = gate_pre * sigma
        act[k, :, pl.ds(0, ff)] = up_pre * sigma * (1.0 + gate_pre * (1.0 - sigma))
        act[k, :, pl.ds(ff, ff)] = active
        cols = pl.ds(pl.multiple_of(k * toks, toks), toks)
        tcat[pl.ds(0, ff), cols] = (active * up_pre).T.astype(BF16)

    def grad_chunk(c):
        whole = gall[c].reshape(parts * toks, cw)
        own[c] = jnp.dot(tcat[pl.ds(0, ff), :], whole, preferred_element_type=F32).astype(BF16)

    def accumulate(c):
        def one(i, carry):
            for n in range(UNROLL):
                k = i * UNROLL + n
                block = gall[c, k].reshape(toks, cw)
                gh[k] = gh[k] + jnp.dot(block, dwt[c], preferred_element_type=F32)
            return carry

        lax.fori_loop(0, parts // UNROLL, one, 0)

    def elementwise(k, carry):
        half = 0.5 * gh[k]
        ggp = half * act[k, :, pl.ds(0, ff)]
        gup = half * act[k, :, pl.ds(ff, ff)]
        cols = pl.ds(pl.multiple_of(k * toks, toks), toks)
        gcat[k, :, :, pl.ds(0, ff)] = ggp.astype(BF16).reshape(ranks, rk, ff)
        gcat[k, :, :, pl.ds(ff, ff)] = gup.astype(BF16).reshape(ranks, rk, ff)
        tcat[pl.ds(0, ff), cols] = ggp.T.astype(BF16)
        tcat[pl.ds(ff, ff), cols] = gup.T.astype(BF16)
        return carry

    def weight_pair(c):
        cols = pl.ds(pl.multiple_of(c * cw, cw), cw)
        whole = nall[:, :, :, cols].reshape(parts * toks, cw)
        both = jnp.dot(tcat[...], whole, preferred_element_type=F32).astype(BF16)
        own[parts + 2 * c] = both[:ff]
        own[parts + 2 * c + 1] = both[ff:]

    def piece(ref, s, h):
        return ref.at[s, pl.ds(h * sub, sub)]

    def up_copy(s, h, src, dst, recv):
        return remote(piece(src, s, h), piece(dst, s, h), up_send.at[s, h], recv.at[s, h], up)

    def down_copy(s, h):
        return remote(piece(fin, s, h), piece(fin, s, h), down_send.at[s, h], fin_recv.at[s, h], down)

    def down_store(s):
        cols = pl.ds(pl.multiple_of(s * cw, cw), cw)
        return pltpu.make_async_copy(fin.at[s], down_out.at[:, cols], osem.at[s % 2])

    def gate_store(s, out):
        here = pl.ds(pl.multiple_of(((s - parts) // 2) * cw, cw), cw)
        return pltpu.make_async_copy(stage_g.at[s % 2], out.at[here], osem.at[2 + s % 2])

    def emit(s):
        @pl.when(s < parts)
        def _():
            @pl.when(s >= 2)
            def _():
                down_store(s - 2).wait()

            down_store(s).start()

        @pl.when(s >= parts)
        def _():
            @pl.when(s >= parts + 2)
            def _():
                gate_store(s - 2, gate_out).wait()

            stage_g[s % 2] = fin[s].T

            @pl.when(s % 2 == 0)
            def _():
                gate_store(s, gate_out).start()

            @pl.when(s % 2 == 1)
            def _():
                gate_store(s, up_out).start()

    def send_own(s):
        @pl.when(outer)
        def _():
            for h in range(SUB):
                @pl.when(center)
                def _():
                    up_copy(s, h, own, fin, fin_recv).start()

                @pl.when(inner)
                def _():
                    up_copy(s, h, own, inc, in_recv).start()

    def settle(s):
        for h in range(SUB):
            up_copy(s, h, own, inc, in_recv).wait_send()

            @pl.when(has_down)
            def _():
                down_copy(s, h).wait_send()

    def reduce_step(z):
        s_in = z - LAG_IN

        @pl.when(has_down & (s_in >= 0) & (s_in < chunks))
        def _():
            for h in range(SUB):
                up_copy(s_in, h, inc, inc, in_recv).wait_recv()
                here = piece(inc, s_in, h)
                here[...] = (piece(own, s_in, h)[...].astype(F32) + here[...].astype(F32)).astype(BF16)

                @pl.when(center)
                def _():
                    up_copy(s_in, h, inc, fin, fin_recv).start()

                @pl.when(inner)
                def _():
                    up_copy(s_in, h, inc, inc, in_recv).start()

        s_fin = z - jnp.where(center, LAG_FIN, LAG_OUT)

        @pl.when((s_fin >= 0) & (s_fin < chunks))
        def _():
            for h in range(SUB):
                down_copy(s_fin, h).wait_recv()
                here = piece(fin, s_fin, h)

                @pl.when(center & has_down)
                def _():
                    here[...] = (piece(inc, s_fin, h)[...].astype(F32) + here[...].astype(F32)).astype(BF16)

                @pl.when(center & outer)
                def _():
                    here[...] = (piece(own, s_fin, h)[...].astype(F32) + here[...].astype(F32)).astype(BF16)

                @pl.when(has_down)
                def _():
                    down_copy(s_fin, h).start()

            emit(s_fin)

        s_old = s_fin - LAG_SEND

        @pl.when((s_old >= 0) & (s_old < chunks))
        def _():
            settle(s_old)

    def pair_copy(j):
        return remote(tbuf.at[(3 - j) % 2], pin.at[j], p_send.at[j], p_recv.at[j], to_p)

    def peer_copy(j):
        return remote(pin.at[j], rsin.at[j - 1], s_send.at[j], s_recv.at[j], {"fs": flip(f, j)})

    def term(owner, c):
        cols = pl.ds(pl.multiple_of(c * cw, cw), cw)
        block = gcat[:, owner].reshape(rows, 2 * ff)
        right = gall[c, pl.ds(0, turn)].reshape(2 * ff, cw)
        return jnp.dot(block, right, preferred_element_type=F32).astype(BF16), cols

    def turn_weights(c, carry):
        here = pl.ds(pl.multiple_of(c * cw, cw), cw)
        gall[c, pl.ds(0, turn)] = wcat[here, :].T.reshape(turn, ranks, rk, cw)
        return carry

    def exit_step(i):
        j = 3 - i // 2

        @pl.when((i >= 0) & (i < 8) & (i % 2 == 0))
        def _():
            @pl.when(j < 2)
            def _():
                pair_copy(j + 2).wait_send()

            def one(i, carry):
                for n in range(UNROLL):
                    value, cols = term(flip(f, j) * 2 + other, i * UNROLL + n)
                    tbuf[(3 - j) % 2, :, cols] = value
                return carry

            lax.fori_loop(0, parts // UNROLL, one, 0)
            pair_copy(j).start()

        @pl.when((i >= 0) & (i < 8) & (i % 2 == 1))
        def _():
            pair_copy(j).wait_recv()

            def one(i, carry):
                for n in range(UNROLL):
                    c = i * UNROLL + n
                    value, cols = term(flip(f, j) * 2 + t, c)
                    total = value.astype(F32) + pin[j, :, cols].astype(F32)
                    gh[c, :, pl.ds(0, cw)] = total
                    pin[j, :, cols] = total.astype(BF16)
                return carry

            lax.fori_loop(0, parts // UNROLL, one, 0)

            @pl.when(j > 0)
            def _():
                peer_copy(j).start()

    def vec_copy(n):
        dev = (to_p, to_a, to_b)[n]
        return remote(gv.at[n], gr.at[n], v_send.at[n], v_recv.at[n], dev)

    def rep_copy(i, incoming=False):
        at = (r - i + reps) % reps if incoming else r
        return remote(grep.at[at], grep.at[at], w_send.at[i], w_recv.at[i], {"rep": (r + i) % reps})

    def reload(k):
        return pltpu.make_async_copy(g_hbm.at[k], tbuf.at[0, pl.ds(k * rk, rk)], lsem.at[3 + k])

    def finish():
        for k in range(parts):
            reload(k).wait()
        for j in (3, 2, 1):
            peer_copy(j).wait_recv()
        gv[0] = jnp.zeros_like(gv[0])

        def one(k, carry):
            here = pl.ds(pl.multiple_of(k * rk, rk), rk)
            grads = jnp.concatenate([gh[c, here, pl.ds(0, cw)] for c in range(parts)], axis=1)
            for j in (2, 1, 0):
                grads = grads + rsin[j, here, :].astype(F32)
            floats = xbuf[k].astype(F32)
            inverse = lax.rsqrt(jnp.mean(floats * floats, axis=-1, keepdims=True) + norm_eps)
            unit = floats * inverse
            gv[0] = gv[0] + jnp.sum(grads * unit, axis=0, keepdims=True)
            scaled = grads * gain_ref[...]
            shift = inverse * jnp.mean(scaled * unit, axis=-1, keepdims=True)
            cot = tbuf[0, here, :].astype(F32)
            xbuf[k] = (cot + inverse * scaled - unit * shift).astype(BF16)
            return carry

        lax.fori_loop(0, parts, one, 0)
        pltpu.make_async_copy(xbuf, gi_out, lsem.at[0]).start()
        vec_copy(0).start()

    def drain(ph):
        def one(k, carry):
            for kind in range(9):
                copy(ph, k, kind).wait_send()
            return carry

        return one

    def tick(q, carry):
        for ph in (0, 1):
            k = q - ph * parts

            @pl.when((k >= 0) & (k < parts))
            def _():
                copy(ph, k, 0, True).wait_recv()
                copy(ph, k, 3).start()
                copy(ph, k, 5).start()
                copy(ph, k, 1, True).wait_recv()
                copy(ph, k, 4).start()
                copy(ph, k, 6).start()

        for ph in (0, 1):
            k = q + AHEAD - ph * parts

            @pl.when((k >= 0) & (k < parts))
            def _():
                if ph == 0:
                    normalise(k)
                issue(ph, k)

        @pl.when(q == 1)
        def _():
            for c in local[1:3] + local[3 + parts:]:
                c.wait()

            def clear(k, carry):
                gh[k] = jnp.zeros_like(gh[k])
                return carry

            lax.fori_loop(0, parts, clear, 0)

        @pl.when((q >= 2) & (q < parts + 2))
        def _():
            dwt[q - 2] = own[2 * parts + q - 2].T

        late = q - 2 - parts

        @pl.when((late >= 0) & (late < parts - 1))
        def _():
            accumulate(late)

        for ph in (0, 1):
            k = q - 1 - ph * parts

            @pl.when((k >= 0) & (k < parts))
            def _():
                copy(ph, k, 3, True).wait_recv()
                copy(ph, k, 8).start()
                copy(ph, k, 4, True).wait_recv()
                copy(ph, k, 7).start()
                for kind in (2, 5, 6, 7, 8):
                    copy(ph, k, kind, True).wait_recv()
                if ph == 0:
                    forward(k)
                else:
                    grad_chunk(k)

        z = q - parts - 1

        @pl.when((z >= 0) & (z < parts))
        def _():
            send_own(z)

        @pl.when((z >= parts) & (z < 2 * parts))
        def _():
            weight_pair(z - parts)
            send_own(2 * z - parts)
            send_own(2 * z - parts + 1)

        reduce_step(z)

        @pl.when(q == 2 * parts)
        def _():
            accumulate(parts - 1)
            lax.fori_loop(0, parts, elementwise, 0)

        @pl.when(q == EXIT_TICK - 1)
        def _():
            for ph in (0, 1):
                lax.fori_loop(0, parts, drain(ph), 0)
            lax.fori_loop(0, parts, turn_weights, 0)

        @pl.when(q == EXIT_TICK + 8)
        def _():
            for j in (1, 0):
                pair_copy(j).wait_send()
            for k in range(parts):
                reload(k).start()

        exit_step(q - EXIT_TICK)

        @pl.when(q == FINISH)
        def _():
            finish()

        for n in (0, 1, 2):
            @pl.when(q == FINISH + 1 + n)
            def _():
                vec_copy(n).wait_recv()
                gv[n + 1] = gv[n] + gr[n]
                if n < 2:
                    vec_copy(n + 1).start()
                else:
                    grep[r] = gv[3]
                    for i in range(1, reps):
                        rep_copy(i).start()

        return carry

    ticks = parts + 1 + chunks + LAG_OUT
    lax.fori_loop(0, ticks, tick, 0)

    for i in range(1, reps):
        rep_copy(i, True).wait_recv()
    total = grep[0]
    for i in range(1, reps):
        total = total + grep[i]
    for n in range(3):
        vec_copy(n).wait_send()
    gv[0] = total
    last = pltpu.make_async_copy(gv.at[0], gg_out, lsem.at[1])
    last.start()

    last_fin = ticks - 1 - parts - 1 - jnp.where(center, LAG_FIN, LAG_OUT)

    def settle_rest(s, carry):
        @pl.when(s > last_fin - LAG_SEND)
        def _():
            settle(s)

        return carry

    lax.fori_loop(chunks - LAG_SEND, chunks, settle_rest, 0)
    for j in (3, 2, 1):
        peer_copy(j).wait_send()
    for i in range(1, reps):
        rep_copy(i).wait_send()
    for s in (parts - 2, parts - 1):
        down_store(s).wait()
    for s in (chunks - 2, chunks - 1):
        gate_store(s, up_out).wait()
    pltpu.make_async_copy(xbuf, gi_out, lsem.at[0]).wait()
    last.wait()


def widen_kernel(factor, *refs):
    arrays, rest = refs[:3], refs[3:5]
    outs, rest_outs = refs[5:8], refs[8:10]
    taken, given, held = refs[10:13], refs[13:16], refs[16:18]
    isem, osem, rsem, wsem = refs[18:]

    def rows(a, i):
        size = arrays[a].shape[0] // PIECES
        return pl.ds(i * size, size)

    def take(a, i):
        return pltpu.make_async_copy(arrays[a].at[rows(a, i)], taken[a].at[rows(a, i)], isem.at[a, i])

    def give(a, i):
        return pltpu.make_async_copy(given[a].at[rows(a, i)], outs[a].at[rows(a, i)], osem.at[a, i])

    order = [(a, i) for a in range(3) for i in range(PIECES)]
    for a, i in order:
        take(a, i).start()
    carried = [pltpu.make_async_copy(rest[n], held[n], rsem.at[n]) for n in range(2)]
    passed = [pltpu.make_async_copy(held[n], rest_outs[n], wsem.at[n]) for n in range(2)]
    for c in carried:
        c.start()
    for a, i in order:
        take(a, i).wait()
        scale = 0.5 * factor if a == 0 else factor
        given[a][rows(a, i), :] = taken[a][rows(a, i), :].astype(F32) * scale
        give(a, i).start()
    for n in range(2):
        carried[n].wait()
        passed[n].start()
    for a, i in order:
        give(a, i).wait()
    for c in passed:
        c.wait()


def shards(tokens_in, norm_gain, gate_weight, up_weight, down_weight, out_grad):
    rows, d = tokens_in.shape
    ff = gate_weight.shape[1]
    reps = lax.axis_size("rep")
    ranks = lax.axis_size("fs") * lax.axis_size("tp")
    factor = float(rows * reps * ranks) ** (-0.5)
    rk, cw = rows // PARTS, d // PARTS
    vmem, anywhere = pl.BlockSpec(memory_space=pltpu.VMEM), pl.BlockSpec(memory_space=pl.ANY)
    dma = pltpu.SemaphoreType.DMA
    chunks = 3 * PARTS
    shape = lambda *s: jax.ShapeDtypeStruct(s, F32)
    half = lambda *s: jax.ShapeDtypeStruct(s, BF16)
    narrow = lambda *s: pltpu.VMEM(s, BF16)
    wide = lambda *s: pltpu.VMEM(s, F32)
    grad_in, grad_gain, grad_down, grad_gate, grad_up = pl.pallas_call(
        lambda *refs: fused_kernel(reps, *refs),
        out_shape=[
            half(PARTS, rk, d), shape(1, d), half(ff, d), half(d, ff), half(d, ff),
        ],
        in_specs=[anywhere, anywhere, vmem, anywhere, anywhere, anywhere],
        out_specs=[anywhere] * 5,
        scratch_shapes=[
            narrow(PARTS, ranks, rk, d), narrow(PARTS, PARTS, ranks, rk, cw),
            narrow(d, 2 * ff), narrow(PARTS, cw, ff),
            wide(PARTS, ranks * rk, 2 * ff), wide(PARTS, ranks * rk, ff),
            narrow(2 * ff, PARTS * ranks * rk), narrow(PARTS, ranks, rk, 2 * ff),
            narrow(chunks, ff, cw), narrow(chunks, ff, cw), narrow(chunks, ff, cw),
            narrow(2, rows, d), narrow(4, rows, d), narrow(3, rows, d), narrow(PARTS, rk, d),
            narrow(2, cw, ff), wide(4, 1, d), wide(3, 1, d), wide(reps, 1, d),
            dma((9, 2 * PARTS)), dma((9, 2 * PARTS)), dma((3 + 2 * PARTS,)),
            dma((chunks, SUB)), dma((chunks, SUB)), dma((chunks, SUB)), dma((chunks, SUB)),
            dma((4,)), dma((4,)), dma((4,)), dma((4,)), dma((3,)), dma((3,)), dma((reps,)), dma((reps,)), dma((4,)),
        ],
        compiler_params=pltpu.CompilerParams(
            collective_id=0, has_side_effects=True, vmem_limit_bytes=63 * 2**20
        ),
        name="fused_backward",
    )(
        tokens_in.reshape(PARTS, rk, d), out_grad.reshape(PARTS, rk, d), norm_gain.reshape(1, d),
        gate_weight, up_weight, down_weight,
    )
    arrays = (grad_down, grad_gate, grad_up)
    outs = [shape(*a.shape) for a in arrays]
    grad_down, grad_gate, grad_up, grad_in, grad_gain = pl.pallas_call(
        lambda *refs: widen_kernel(factor, *refs),
        out_shape=outs + [half(rows, d), shape(1, d)],
        in_specs=[anywhere] * 5,
        out_specs=[anywhere] * 5,
        scratch_shapes=[narrow(*a.shape) for a in arrays] + [wide(*a.shape) for a in arrays] + [
            narrow(rows, d), wide(1, d), dma((3, PIECES)), dma((3, PIECES)), dma((2,)), dma((2,)),
        ],
        compiler_params=pltpu.CompilerParams(vmem_limit_bytes=63 * 2**20),
        name="widen",
    )(grad_down, grad_gate, grad_up, grad_in.reshape(rows, d), grad_gain)
    return (grad_in, grad_gain.reshape(d), grad_gate, grad_up, grad_down)


def solution(mesh):
    spread = ("fs", "tp")
    in_specs = (
        P(("rep", "fs", "tp"), None), P(), P(None, spread), P(None, spread), P(spread, None),
        P(("rep", "fs", "tp"), None),
    )
    out_specs = (
        P(("rep", "fs", "tp"), None), P(), P(None, spread), P(None, spread), P(spread, None),
    )
    return jax.shard_map(shards, mesh=mesh, in_specs=in_specs, out_specs=out_specs, check_vma=False)
```

```python
import jax
import jax.numpy as jnp
from jax import lax
from jax.experimental import pallas as pl
from jax.experimental.pallas import tpu as pltpu
from jax.sharding import PartitionSpec as P

norm_eps = 1e-06
MESH = pl.DeviceIdType.MESH
F32, BF16 = jnp.float32, jnp.bfloat16
NT = (((1,), (1,)), ((), ()))
PARTS = 8
AHEAD = 2
PIECES = 4
SUB = 2
LAG_IN = 1
LAG_FIN = 2
LAG_OUT = 6
EXIT_TICK = 2 * PARTS + 2
UNROLL = 4
FINISH = 31


def flip(f, j):
    return (f % 2 + j % 2) % 2 + 2 * ((f // 2 + j // 2) % 2)


def remote(src, dst, send, recv, dev):
    return pltpu.make_async_remote_copy(
        src_ref=src, dst_ref=dst, send_sem=send, recv_sem=recv, device_id=dev, device_id_type=MESH
    )


def fused_kernel(
    reps,
    x_hbm, g_hbm, gain_ref, gw_hbm, uw_hbm, dw_hbm,
    gi_out, gg_out, down_out, gate_out, up_out,
    nall, gall, wcat, dwt, act, gh, tcat, gcat, own, inc, fin,
    tbuf, pin, rsin, xbuf, stage_g, gv, gr, grep,
    ssem, rsem, lsem, up_send, in_recv, down_send, fin_recv,
    p_send, p_recv, s_send, s_recv, v_send, v_recv, w_send, w_recv, osem,
):
    f, t, r = lax.axis_index("fs"), lax.axis_index("tp"), lax.axis_index("rep")
    other = 1 - t
    parts, rk, d = xbuf.shape
    rows = parts * rk
    ff = dwt.shape[2]
    cw = d // parts
    ranks = gcat.shape[1]
    toks = ranks * rk
    chunks = 3 * parts
    sub = ff // SUB
    ticks = parts + 1 + chunks + LAG_OUT
    turn = 2 * ff // toks

    middle = reps // 2
    sign = 1 - 2 * (r // middle)
    up, down = {"rep": r + sign}, {"rep": (r - sign + reps) % reps}
    right = r // middle
    depth = (1 - right) * (middle - 1 - r) + right * (r - middle)
    center, outer = depth == 0, depth == middle - 1
    inner, has_down = depth > 0, depth < middle - 1
    to_a, to_b, to_p = {"fs": flip(f, 1)}, {"fs": flip(f, 2)}, {"tp": other}

    barrier = pltpu.get_barrier_semaphore()
    for dev in (to_a, to_b, {"fs": flip(f, 3)}, to_p):
        pl.semaphore_signal(barrier, inc=1, device_id=dev, device_id_type=MESH)
    for i in range(1, reps):
        pl.semaphore_signal(barrier, inc=1, device_id={"rep": (r + i) % reps}, device_id_type=MESH)

    def pos(j, core):
        return flip(f, j) * 2 + core

    me = pos(0, t)

    def loads():
        out = [pltpu.make_async_copy(x_hbm, xbuf, lsem.at[0])]
        out.append(pltpu.make_async_copy(gw_hbm, wcat.at[:, pl.ds(0, ff)], lsem.at[1]))
        out.append(pltpu.make_async_copy(uw_hbm, wcat.at[:, pl.ds(ff, ff)], lsem.at[2]))
        for c in range(parts):
            cols = pl.ds(c * cw, cw)
            out.append(pltpu.make_async_copy(g_hbm.at[:, :, cols], gall.at[c, :, me], lsem.at[3 + c]))
        for c in range(parts):
            cols = pl.ds(c * cw, cw)
            out.append(pltpu.make_async_copy(dw_hbm.at[:, cols], own.at[2 * parts + c], lsem.at[3 + parts + c]))
        return out

    local = loads()
    for c in local:
        c.start()

    def slot(ph, k, p, part=0):
        if ph == 0:
            ref = nall.at[k, p]
            size = rk // 2
        else:
            ref = gall.at[k, :, p]
            size = parts // 2
        if part == 0:
            return ref
        return ref.at[pl.ds((part - 1) * size, size)]

    def copy(ph, k, kind, incoming=False):
        sems = (ssem.at[kind, ph], rsem.at[kind, k])
        core = other if incoming else t
        if kind == 0:
            ref, dev = slot(ph, k, pos(1, t) if incoming else me), to_a
        elif kind == 1:
            ref, dev = slot(ph, k, pos(2, t) if incoming else me), to_b
        elif kind == 2:
            ref, dev = slot(ph, k, pos(0, core)), to_p
        elif kind == 3:
            ref, dev = slot(ph, k, pos(3, t) if incoming else pos(1, t), 2), to_b
        elif kind == 4:
            ref, dev = slot(ph, k, pos(3, t) if incoming else pos(2, t), 1), to_a
        elif kind == 5:
            ref, dev = slot(ph, k, pos(1, core)), to_p
        elif kind == 6:
            ref, dev = slot(ph, k, pos(2, core)), to_p
        else:
            ref, dev = slot(ph, k, pos(3, core), kind - 6), to_p
        return remote(ref, ref, *sems, dev)

    def normalise(k):
        floats = xbuf[k].astype(F32)
        inverse = lax.rsqrt(jnp.mean(floats * floats, axis=-1, keepdims=True) + norm_eps)
        nall[k, me] = (floats * inverse * gain_ref[...]).astype(BF16)

    def issue(ph, k):
        for kind in (0, 1, 2):
            copy(ph, k, kind).start()

    local[0].wait()
    for k in range(AHEAD):
        normalise(k)
    pl.semaphore_wait(barrier, 3 + reps)
    for k in range(AHEAD):
        issue(0, k)
    for c in local[3:3 + parts]:
        c.wait()

    def forward(k):
        block = nall[k].reshape(toks, d)
        pre = jnp.dot(block, wcat[...], preferred_element_type=F32)
        gate_pre, up_pre = pre[:, :ff], pre[:, ff:]
        sigma = jax.nn.sigmoid(gate_pre)
        active = gate_pre * sigma
        act[k, :, pl.ds(0, ff)] = up_pre * sigma * (1.0 + gate_pre * (1.0 - sigma))
        act[k, :, pl.ds(ff, ff)] = active
        cols = pl.ds(pl.multiple_of(k * toks, toks), toks)
        tcat[pl.ds(0, ff), cols] = (active * up_pre).T.astype(BF16)

    def grad_chunk(c):
        whole = gall[c].reshape(parts * toks, cw)
        own[c] = jnp.dot(tcat[pl.ds(0, ff), :], whole, preferred_element_type=F32).astype(BF16)

    def accumulate(c):
        def one(i, carry):
            for n in range(UNROLL):
                k = i * UNROLL + n
                block = gall[c, k].reshape(toks, cw)
                gh[k] = gh[k] + jnp.dot(block, dwt[c], preferred_element_type=F32)
            return carry

        lax.fori_loop(0, parts // UNROLL, one, 0)

    def elementwise(k, carry):
        half = 0.5 * gh[k]
        ggp = half * act[k, :, pl.ds(0, ff)]
        gup = half * act[k, :, pl.ds(ff, ff)]
        cols = pl.ds(pl.multiple_of(k * toks, toks), toks)
        gcat[k, :, :, pl.ds(0, ff)] = ggp.astype(BF16).reshape(ranks, rk, ff)
        gcat[k, :, :, pl.ds(ff, ff)] = gup.astype(BF16).reshape(ranks, rk, ff)
        tcat[pl.ds(0, ff), cols] = ggp.T.astype(BF16)
        tcat[pl.ds(ff, ff), cols] = gup.T.astype(BF16)
        return carry

    def weight_pair(c):
        cols = pl.ds(pl.multiple_of(c * cw, cw), cw)
        whole = nall[:, :, :, cols].reshape(parts * toks, cw)
        both = jnp.dot(tcat[...], whole, preferred_element_type=F32).astype(BF16)
        own[parts + 2 * c] = both[:ff]
        own[parts + 2 * c + 1] = both[ff:]

    def piece(ref, s, h):
        return ref.at[s, pl.ds(h * sub, sub)]

    def up_copy(s, h, src, dst, recv):
        return remote(piece(src, s, h), piece(dst, s, h), up_send.at[0], recv.at[s, h], up)

    def down_copy(s, h):
        return remote(piece(fin, s, h), piece(fin, s, h), down_send.at[0], fin_recv.at[s, h], down)

    def down_store(s):
        cols = pl.ds(pl.multiple_of(s * cw, cw), cw)
        return pltpu.make_async_copy(fin.at[s], down_out.at[:, cols], osem.at[s % 2])

    def gate_store(s, out):
        here = pl.ds(pl.multiple_of(((s - parts) // 2) * cw, cw), cw)
        return pltpu.make_async_copy(stage_g.at[s % 2], out.at[here], osem.at[2 + s % 2])

    def emit(s):
        @pl.when(s < parts)
        def _():
            @pl.when(s >= 2)
            def _():
                down_store(s - 2).wait()

            down_store(s).start()

        @pl.when(s >= parts)
        def _():
            @pl.when(s >= parts + 2)
            def _():
                gate_store(s - 2, gate_out).wait()

            stage_g[s % 2] = fin[s].T

            @pl.when(s % 2 == 0)
            def _():
                gate_store(s, gate_out).start()

            @pl.when(s % 2 == 1)
            def _():
                gate_store(s, up_out).start()

    def send_own(s):
        @pl.when(outer)
        def _():
            for h in range(SUB):
                @pl.when(center)
                def _():
                    up_copy(s, h, own, fin, fin_recv).start()

                @pl.when(inner)
                def _():
                    up_copy(s, h, own, inc, in_recv).start()

    def take_in(s, h):
        @pl.when(has_down & (s >= 0) & (s < chunks))
        def _():
            up_copy(s, h, inc, inc, in_recv).wait_recv()
            here = piece(inc, s, h)
            here[...] = (piece(own, s, h)[...].astype(F32) + here[...].astype(F32)).astype(BF16)

            @pl.when(center)
            def _():
                up_copy(s, h, inc, fin, fin_recv).start()

            @pl.when(inner)
            def _():
                up_copy(s, h, inc, inc, in_recv).start()

    def take_fin(s, h):
        down_copy(s, h).wait_recv()
        here = piece(fin, s, h)

        @pl.when(center & has_down)
        def _():
            here[...] = (piece(inc, s, h)[...].astype(F32) + here[...].astype(F32)).astype(BF16)

        @pl.when(center & outer)
        def _():
            here[...] = (piece(own, s, h)[...].astype(F32) + here[...].astype(F32)).astype(BF16)

        @pl.when(has_down)
        def _():
            down_copy(s, h).start()

    def reduce_step(z):
        for h in range(SUB):
            take_in(z - LAG_IN, h)

        s_mid = z - LAG_FIN

        @pl.when(center & has_down & (s_mid >= 0) & (s_mid < chunks))
        def _():
            for h in range(SUB - 1):
                take_fin(s_mid, h)

        s_fin = z - LAG_OUT

        @pl.when((s_fin >= 0) & (s_fin < chunks) & (outer | inner))
        def _():
            for h in range(SUB):
                take_fin(s_fin, h)
            emit(s_fin)

    def reduce_rest(z):
        s_mid = z - LAG_FIN - 1

        @pl.when(center & has_down & (s_mid >= 0) & (s_mid < chunks))
        def _():
            take_fin(s_mid, SUB - 1)
            emit(s_mid)

    def pair_copy(j):
        return remote(tbuf.at[(3 - j) % 2], pin.at[j], p_send.at[j], p_recv.at[j], to_p)

    def peer_copy(j):
        return remote(pin.at[j], rsin.at[j - 1], s_send.at[j], s_recv.at[j], {"fs": flip(f, j)})

    def term(owner, c):
        cols = pl.ds(pl.multiple_of(c * cw, cw), cw)
        block = gcat[:, owner].reshape(rows, 2 * ff)
        right = gall[c, pl.ds(0, turn)].reshape(2 * ff, cw)
        return jnp.dot(block, right, preferred_element_type=F32).astype(BF16), cols

    def turn_weights(c, carry):
        here = pl.ds(pl.multiple_of(c * cw, cw), cw)
        gall[c, pl.ds(0, turn)] = wcat[here, :].T.reshape(turn, ranks, rk, cw)
        return carry

    def exit_step(i):
        j = 3 - i // 2

        @pl.when((i >= 0) & (i < 8) & (i % 2 == 0))
        def _():
            @pl.when(j < 2)
            def _():
                pair_copy(j + 2).wait_send()

            def one(i, carry):
                for n in range(UNROLL):
                    value, cols = term(flip(f, j) * 2 + other, i * UNROLL + n)
                    tbuf[(3 - j) % 2, :, cols] = value
                return carry

            lax.fori_loop(0, parts // UNROLL, one, 0)
            pair_copy(j).start()

        @pl.when((i >= 0) & (i < 8) & (i % 2 == 1))
        def _():
            pair_copy(j).wait_recv()

            def one(i, carry):
                for n in range(UNROLL):
                    c = i * UNROLL + n
                    value, cols = term(flip(f, j) * 2 + t, c)
                    total = value.astype(F32) + pin[j, :, cols].astype(F32)
                    gh[c, :, pl.ds(0, cw)] = total
                    pin[j, :, cols] = total.astype(BF16)
                return carry

            lax.fori_loop(0, parts // UNROLL, one, 0)

            @pl.when(j > 0)
            def _():
                peer_copy(j).start()

    def vec_copy(n):
        dev = (to_p, to_a, to_b)[n]
        return remote(gv.at[n], gr.at[n], v_send.at[n], v_recv.at[n], dev)

    def rep_copy(i, incoming=False):
        at = (r - i + reps) % reps if incoming else r
        return remote(grep.at[at], grep.at[at], w_send.at[i], w_recv.at[i], {"rep": (r + i) % reps})

    def reload(k):
        return pltpu.make_async_copy(g_hbm.at[k], tbuf.at[0, pl.ds(k * rk, rk)], lsem.at[3 + k])

    def finish():
        for k in range(parts):
            reload(k).wait()
        for j in (3, 2, 1):
            peer_copy(j).wait_recv()
        gv[0] = jnp.zeros_like(gv[0])

        def one(k, carry):
            here = pl.ds(pl.multiple_of(k * rk, rk), rk)
            grads = jnp.concatenate([gh[c, here, pl.ds(0, cw)] for c in range(parts)], axis=1)
            for j in (2, 1, 0):
                grads = grads + rsin[j, here, :].astype(F32)
            floats = xbuf[k].astype(F32)
            inverse = lax.rsqrt(jnp.mean(floats * floats, axis=-1, keepdims=True) + norm_eps)
            unit = floats * inverse
            gv[0] = gv[0] + jnp.sum(grads * unit, axis=0, keepdims=True)
            scaled = grads * gain_ref[...]
            shift = inverse * jnp.mean(scaled * unit, axis=-1, keepdims=True)
            cot = tbuf[0, here, :].astype(F32)
            xbuf[k] = (cot + inverse * scaled - unit * shift).astype(BF16)
            return carry

        lax.fori_loop(0, parts, one, 0)
        pltpu.make_async_copy(xbuf, gi_out, lsem.at[0]).start()
        vec_copy(0).start()

    def drain(ph):
        places = (me, me, me, pos(1, t), pos(2, t), pos(1, t), pos(2, t), pos(3, t), pos(3, t))
        for kind, p in enumerate(places):
            part = {3: 2, 4: 1, 7: 1, 8: 2}.get(kind, 0)
            if ph == 0:
                size = rk // 2 if part else rk
                ref = nall.at[:, p, pl.ds(max(part - 1, 0) * size, size)]
            else:
                size = parts // 2 if part else parts
                ref = gall.at[:, pl.ds(max(part - 1, 0) * size, size), p]
            remote(ref, ref, ssem.at[kind, ph], rsem.at[kind, 0], to_p).wait_send()

    def gain_store():
        return pltpu.make_async_copy(gv.at[0], gg_out, lsem.at[1])

    def gain_total():
        for i in range(1, reps):
            rep_copy(i, True).wait_recv()
        total = grep[0]
        for i in range(1, reps):
            total = total + grep[i]
        for n in range(3):
            vec_copy(n).wait_send()
        gv[0] = total
        gain_store().start()

    def tick(q, carry):
        for ph in (0, 1):
            k = q - ph * parts

            @pl.when((k >= 0) & (k < parts))
            def _():
                copy(ph, k, 0, True).wait_recv()
                copy(ph, k, 3).start()
                copy(ph, k, 5).start()
                copy(ph, k, 1, True).wait_recv()
                copy(ph, k, 4).start()
                copy(ph, k, 6).start()

        for ph in (0, 1):
            k = q + AHEAD - ph * parts

            @pl.when((k >= 0) & (k < parts))
            def _():
                if ph == 0:
                    normalise(k)
                issue(ph, k)

        @pl.when(q == 1)
        def _():
            for c in local[1:3] + local[3 + parts:]:
                c.wait()

            def clear(k, carry):
                gh[k] = jnp.zeros_like(gh[k])
                return carry

            lax.fori_loop(0, parts, clear, 0)

        @pl.when((q >= 2) & (q < parts + 2))
        def _():
            dwt[q - 2] = own[2 * parts + q - 2].T

        late = q - 2 - parts

        @pl.when((late >= 0) & (late < parts - 1))
        def _():
            accumulate(late)

        z = q - parts - 1
        reduce_rest(z)

        for ph in (0, 1):
            k = q - 1 - ph * parts

            @pl.when((k >= 0) & (k < parts))
            def _():
                copy(ph, k, 3, True).wait_recv()
                copy(ph, k, 8).start()
                copy(ph, k, 4, True).wait_recv()
                copy(ph, k, 7).start()
                for kind in (2, 5, 6, 7, 8):
                    copy(ph, k, kind, True).wait_recv()
                if ph == 0:
                    forward(k)
                else:
                    grad_chunk(k)

        @pl.when((z >= 0) & (z < parts))
        def _():
            send_own(z)

        @pl.when((z >= parts) & (z < 2 * parts))
        def _():
            weight_pair(z - parts)
            send_own(2 * z - parts)
            send_own(2 * z - parts + 1)

        reduce_step(z)

        @pl.when(q == 2 * parts)
        def _():
            accumulate(parts - 1)
            lax.fori_loop(0, parts, elementwise, 0)

        @pl.when(q == EXIT_TICK - 1)
        def _():
            drain(0)
            drain(1)
            lax.fori_loop(0, parts, turn_weights, 0)

        @pl.when(q == EXIT_TICK + 8)
        def _():
            for j in (1, 0):
                pair_copy(j).wait_send()
            for k in range(parts):
                reload(k).start()

        exit_step(q - EXIT_TICK)

        @pl.when(q == FINISH)
        def _():
            finish()

        for n in (0, 1, 2):
            @pl.when(q == FINISH + 1 + n)
            def _():
                vec_copy(n).wait_recv()
                gv[n + 1] = gv[n] + gr[n]
                if n < 2:
                    vec_copy(n + 1).start()
                else:
                    grep[r] = gv[3]
                    for i in range(1, reps):
                        rep_copy(i).start()

        @pl.when(q == ticks - 1)
        def _():
            gain_total()

        return carry

    lax.fori_loop(0, ticks, tick, 0)

    remote(own, inc, up_send.at[0], in_recv.at[0, 0], up).wait_send()

    @pl.when(has_down)
    def _():
        remote(fin, fin, down_send.at[0], fin_recv.at[0, 0], down).wait_send()

    for j in (3, 2, 1):
        peer_copy(j).wait_send()
    for i in range(1, reps):
        rep_copy(i).wait_send()
    for s in (parts - 2, parts - 1):
        down_store(s).wait()
    for s in (chunks - 2, chunks - 1):
        gate_store(s, up_out).wait()
    pltpu.make_async_copy(xbuf, gi_out, lsem.at[0]).wait()
    gain_store().wait()


def widen_kernel(factor, *refs):
    arrays, rest = refs[:3], refs[3:5]
    outs, rest_outs = refs[5:8], refs[8:10]
    taken, given, held = refs[10:13], refs[13:16], refs[16:18]
    isem, osem, rsem, wsem = refs[18:]

    def rows(a, i):
        size = arrays[a].shape[0] // PIECES
        return pl.ds(i * size, size)

    def take(a, i):
        return pltpu.make_async_copy(arrays[a].at[rows(a, i)], taken[a].at[rows(a, i)], isem.at[a, i])

    def give(a, i):
        return pltpu.make_async_copy(given[a].at[rows(a, i)], outs[a].at[rows(a, i)], osem.at[a, i])

    order = [(a, i) for a in range(3) for i in range(PIECES)]
    for a, i in order:
        take(a, i).start()
    carried = [pltpu.make_async_copy(rest[n], held[n], rsem.at[n]) for n in range(2)]
    passed = [pltpu.make_async_copy(held[n], rest_outs[n], wsem.at[n]) for n in range(2)]
    for c in carried:
        c.start()
    for a, i in order:
        take(a, i).wait()
        scale = 0.5 * factor if a == 0 else factor
        given[a][rows(a, i), :] = taken[a][rows(a, i), :].astype(F32) * scale
        give(a, i).start()
    for n in range(2):
        carried[n].wait()
        passed[n].start()
    for a, i in order:
        give(a, i).wait()
    for c in passed:
        c.wait()


def shards(tokens_in, norm_gain, gate_weight, up_weight, down_weight, out_grad):
    rows, d = tokens_in.shape
    ff = gate_weight.shape[1]
    reps = lax.axis_size("rep")
    ranks = lax.axis_size("fs") * lax.axis_size("tp")
    factor = float(rows * reps * ranks) ** (-0.5)
    rk, cw = rows // PARTS, d // PARTS
    vmem, anywhere = pl.BlockSpec(memory_space=pltpu.VMEM), pl.BlockSpec(memory_space=pl.ANY)
    dma = pltpu.SemaphoreType.DMA
    chunks = 3 * PARTS
    shape = lambda *s: jax.ShapeDtypeStruct(s, F32)
    half = lambda *s: jax.ShapeDtypeStruct(s, BF16)
    narrow = lambda *s: pltpu.VMEM(s, BF16)
    wide = lambda *s: pltpu.VMEM(s, F32)
    grad_in, grad_gain, grad_down, grad_gate, grad_up = pl.pallas_call(
        lambda *refs: fused_kernel(reps, *refs),
        out_shape=[
            half(PARTS, rk, d), shape(1, d), half(ff, d), half(d, ff), half(d, ff),
        ],
        in_specs=[anywhere, anywhere, vmem, anywhere, anywhere, anywhere],
        out_specs=[anywhere] * 5,
        scratch_shapes=[
            narrow(PARTS, ranks, rk, d), narrow(PARTS, PARTS, ranks, rk, cw),
            narrow(d, 2 * ff), narrow(PARTS, cw, ff),
            wide(PARTS, ranks * rk, 2 * ff), wide(PARTS, ranks * rk, ff),
            narrow(2 * ff, PARTS * ranks * rk), narrow(PARTS, ranks, rk, 2 * ff),
            narrow(chunks, ff, cw), narrow(chunks, ff, cw), narrow(chunks, ff, cw),
            narrow(2, rows, d), narrow(4, rows, d), narrow(3, rows, d), narrow(PARTS, rk, d),
            narrow(2, cw, ff), wide(4, 1, d), wide(3, 1, d), wide(reps, 1, d),
            dma((9, 2)), dma((9, PARTS)), dma((3 + 2 * PARTS,)),
            dma((1,)), dma((chunks, SUB)), dma((1,)), dma((chunks, SUB)),
            dma((4,)), dma((4,)), dma((4,)), dma((4,)), dma((3,)), dma((3,)), dma((reps,)), dma((reps,)), dma((4,)),
        ],
        compiler_params=pltpu.CompilerParams(
            collective_id=0, has_side_effects=True, vmem_limit_bytes=63 * 2**20
        ),
        name="fused_backward",
    )(
        tokens_in.reshape(PARTS, rk, d), out_grad.reshape(PARTS, rk, d), norm_gain.reshape(1, d),
        gate_weight, up_weight, down_weight,
    )
    arrays = (grad_down, grad_gate, grad_up)
    outs = [shape(*a.shape) for a in arrays]
    grad_down, grad_gate, grad_up, grad_in, grad_gain = pl.pallas_call(
        lambda *refs: widen_kernel(factor, *refs),
        out_shape=outs + [half(rows, d), shape(1, d)],
        in_specs=[anywhere] * 5,
        out_specs=[anywhere] * 5,
        scratch_shapes=[narrow(*a.shape) for a in arrays] + [wide(*a.shape) for a in arrays] + [
            narrow(rows, d), wide(1, d), dma((3, PIECES)), dma((3, PIECES)), dma((2,)), dma((2,)),
        ],
        compiler_params=pltpu.CompilerParams(vmem_limit_bytes=63 * 2**20),
        name="widen",
    )(grad_down, grad_gate, grad_up, grad_in.reshape(rows, d), grad_gain)
    return (grad_in, grad_gain.reshape(d), grad_gate, grad_up, grad_down)


def solution(mesh):
    spread = ("fs", "tp")
    in_specs = (
        P(("rep", "fs", "tp"), None), P(), P(None, spread), P(None, spread), P(spread, None),
        P(("rep", "fs", "tp"), None),
    )
    out_specs = (
        P(("rep", "fs", "tp"), None), P(), P(None, spread), P(None, spread), P(spread, None),
    )
    return jax.shard_map(shards, mesh=mesh, in_specs=in_specs, out_specs=out_specs, check_vma=False)
```

```python
import jax
import jax.numpy as jnp
from jax import lax
from jax.experimental import pallas as pl
from jax.experimental.pallas import tpu as pltpu
from jax.sharding import PartitionSpec as P

norm_eps = 1e-06
MESH = pl.DeviceIdType.MESH
F32, BF16 = jnp.float32, jnp.bfloat16
NT = (((1,), (1,)), ((), ()))
PARTS = 8
AHEAD = 2
PIECES = 2
SUB = 2
LAG_IN = 1
LAG_FIN = 2
LAG_OUT = 6
EXIT_TICK = 2 * PARTS + 2
UNROLL = 8
FINISH = 31


def flip(f, j):
    return (f % 2 + j % 2) % 2 + 2 * ((f // 2 + j // 2) % 2)


def remote(src, dst, send, recv, dev):
    return pltpu.make_async_remote_copy(
        src_ref=src, dst_ref=dst, send_sem=send, recv_sem=recv, device_id=dev, device_id_type=MESH
    )


def fused_kernel(
    reps,
    x_hbm, g_hbm, gain_ref, gw_hbm, uw_hbm, dw_hbm,
    gi_out, gg_out, down_out, gate_out, up_out,
    nall, gall, wcat, dwt, act, gh, tcat, gcat, own, inc, fin,
    tbuf, pin, rsin, xbuf, stage_g, gv, gr, grep,
    ssem, rsem, lsem, up_send, in_recv, down_send, fin_recv,
    p_send, p_recv, s_send, s_recv, v_send, v_recv, w_send, w_recv, osem,
):
    f, t, r = lax.axis_index("fs"), lax.axis_index("tp"), lax.axis_index("rep")
    other = 1 - t
    parts, rk, d = xbuf.shape
    rows = parts * rk
    ff = dwt.shape[2]
    cw = d // parts
    ranks = gcat.shape[1]
    toks = ranks * rk
    chunks = 3 * parts
    sub = ff // SUB
    ticks = parts + 1 + chunks + LAG_OUT
    turn = 2 * ff // toks

    middle = reps // 2
    sign = 1 - 2 * (r // middle)
    up, down = {"rep": r + sign}, {"rep": (r - sign + reps) % reps}
    right = r // middle
    depth = (1 - right) * (middle - 1 - r) + right * (r - middle)
    center, outer = depth == 0, depth == middle - 1
    inner, has_down = depth > 0, depth < middle - 1
    to_a, to_b, to_p = {"fs": flip(f, 1)}, {"fs": flip(f, 2)}, {"tp": other}

    barrier = pltpu.get_barrier_semaphore()
    for dev in (to_a, to_b, {"fs": flip(f, 3)}, to_p):
        pl.semaphore_signal(barrier, inc=1, device_id=dev, device_id_type=MESH)
    for i in range(1, reps):
        pl.semaphore_signal(barrier, inc=1, device_id={"rep": (r + i) % reps}, device_id_type=MESH)

    def pos(j, core):
        return flip(f, j) * 2 + core

    me = pos(0, t)

    def loads():
        out = [pltpu.make_async_copy(x_hbm, xbuf, lsem.at[0])]
        out.append(pltpu.make_async_copy(gw_hbm, wcat.at[:, pl.ds(0, ff)], lsem.at[1]))
        out.append(pltpu.make_async_copy(uw_hbm, wcat.at[:, pl.ds(ff, ff)], lsem.at[2]))
        for c in range(parts):
            cols = pl.ds(c * cw, cw)
            out.append(pltpu.make_async_copy(g_hbm.at[:, :, cols], gall.at[c, :, me], lsem.at[3 + c]))
        for c in range(parts):
            cols = pl.ds(c * cw, cw)
            out.append(pltpu.make_async_copy(dw_hbm.at[:, cols], own.at[2 * parts + c], lsem.at[3 + parts + c]))
        return out

    local = loads()
    for c in local:
        c.start()

    def slot(ph, k, p, part=0):
        if ph == 0:
            ref = nall.at[k, p]
            size = rk // 2
        else:
            ref = gall.at[k, :, p]
            size = parts // 2
        if part == 0:
            return ref
        return ref.at[pl.ds((part - 1) * size, size)]

    def copy(ph, k, kind, incoming=False):
        sems = (ssem.at[kind, ph], rsem.at[kind, k])
        core = other if incoming else t
        if kind == 0:
            ref, dev = slot(ph, k, pos(1, t) if incoming else me), to_a
        elif kind == 1:
            ref, dev = slot(ph, k, pos(2, t) if incoming else me), to_b
        elif kind == 2:
            ref, dev = slot(ph, k, pos(0, core)), to_p
        elif kind == 3:
            ref, dev = slot(ph, k, pos(3, t) if incoming else pos(1, t), 2), to_b
        elif kind == 4:
            ref, dev = slot(ph, k, pos(3, t) if incoming else pos(2, t), 1), to_a
        elif kind == 5:
            ref, dev = slot(ph, k, pos(1, core)), to_p
        elif kind == 6:
            ref, dev = slot(ph, k, pos(2, core)), to_p
        else:
            ref, dev = slot(ph, k, pos(3, core), kind - 6), to_p
        return remote(ref, ref, *sems, dev)

    def normalise(k):
        floats = xbuf[k].astype(F32)
        inverse = lax.rsqrt(jnp.mean(floats * floats, axis=-1, keepdims=True) + norm_eps)
        nall[k, me] = (floats * inverse * gain_ref[...]).astype(BF16)

    def issue(ph, k):
        for kind in (0, 1, 2):
            copy(ph, k, kind).start()

    local[0].wait()
    for k in range(AHEAD):
        normalise(k)
    pl.semaphore_wait(barrier, 3 + reps)
    for k in range(AHEAD):
        issue(0, k)
    for c in local[3:3 + parts]:
        c.wait()

    def forward(k):
        block = nall[k].reshape(toks, d)
        pre = jnp.dot(block, wcat[...], preferred_element_type=F32)
        gate_pre, up_pre = pre[:, :ff], pre[:, ff:]
        sigma = jax.nn.sigmoid(gate_pre)
        active = gate_pre * sigma
        act[k, :, pl.ds(0, ff)] = up_pre * sigma * (1.0 + gate_pre * (1.0 - sigma))
        act[k, :, pl.ds(ff, ff)] = active
        cols = pl.ds(pl.multiple_of(k * toks, toks), toks)
        tcat[pl.ds(0, ff), cols] = (active * up_pre).T.astype(BF16)

    def grad_chunk(c):
        whole = gall[c].reshape(parts * toks, cw)
        own[c] = jnp.dot(tcat[pl.ds(0, ff), :], whole, preferred_element_type=F32).astype(BF16)

    def accumulate(c):
        def one(i, carry):
            for n in range(UNROLL):
                k = i * UNROLL + n
                block = gall[c, k].reshape(toks, cw)
                gh[k] = gh[k] + jnp.dot(block, dwt[c], preferred_element_type=F32)
            return carry

        lax.fori_loop(0, parts // UNROLL, one, 0)

    def elementwise(k, carry):
        half = 0.5 * gh[k]
        ggp = half * act[k, :, pl.ds(0, ff)]
        gup = half * act[k, :, pl.ds(ff, ff)]
        cols = pl.ds(pl.multiple_of(k * toks, toks), toks)
        gcat[k, :, :, pl.ds(0, ff)] = ggp.astype(BF16).reshape(ranks, rk, ff)
        gcat[k, :, :, pl.ds(ff, ff)] = gup.astype(BF16).reshape(ranks, rk, ff)
        tcat[pl.ds(0, ff), cols] = ggp.T.astype(BF16)
        tcat[pl.ds(ff, ff), cols] = gup.T.astype(BF16)
        return carry

    def weight_pair(c):
        cols = pl.ds(pl.multiple_of(c * cw, cw), cw)
        whole = nall[:, :, :, cols].reshape(parts * toks, cw)
        both = jnp.dot(tcat[...], whole, preferred_element_type=F32).astype(BF16)
        own[parts + 2 * c] = both[:ff]
        own[parts + 2 * c + 1] = both[ff:]

    def piece(ref, s, h):
        return ref.at[s, pl.ds(h * sub, sub)]

    def up_copy(s, h, src, dst, recv):
        return remote(piece(src, s, h), piece(dst, s, h), up_send.at[0], recv.at[s, h], up)

    def down_copy(s, h):
        return remote(piece(fin, s, h), piece(fin, s, h), down_send.at[0], fin_recv.at[s, h], down)

    def down_store(s):
        cols = pl.ds(pl.multiple_of(s * cw, cw), cw)
        return pltpu.make_async_copy(fin.at[s], down_out.at[:, cols], osem.at[s % 2])

    def gate_store(s, out):
        here = pl.ds(pl.multiple_of(((s - parts) // 2) * cw, cw), cw)
        return pltpu.make_async_copy(stage_g.at[s % 2], out.at[here], osem.at[2 + s % 2])

    def emit(s):
        @pl.when(s < parts)
        def _():
            @pl.when(s >= 2)
            def _():
                down_store(s - 2).wait()

            down_store(s).start()

        @pl.when(s >= parts)
        def _():
            @pl.when(s >= parts + 2)
            def _():
                gate_store(s - 2, gate_out).wait()

            stage_g[s % 2] = fin[s].T

            @pl.when(s % 2 == 0)
            def _():
                gate_store(s, gate_out).start()

            @pl.when(s % 2 == 1)
            def _():
                gate_store(s, up_out).start()

    def send_own(s):
        @pl.when(outer)
        def _():
            for h in range(SUB):
                @pl.when(center)
                def _():
                    up_copy(s, h, own, fin, fin_recv).start()

                @pl.when(inner)
                def _():
                    up_copy(s, h, own, inc, in_recv).start()

    def take_in(s, h):
        @pl.when(has_down & (s >= 0) & (s < chunks))
        def _():
            up_copy(s, h, inc, inc, in_recv).wait_recv()
            here = piece(inc, s, h)
            here[...] = (piece(own, s, h)[...].astype(F32) + here[...].astype(F32)).astype(BF16)

            @pl.when(center)
            def _():
                up_copy(s, h, inc, fin, fin_recv).start()

            @pl.when(inner)
            def _():
                up_copy(s, h, inc, inc, in_recv).start()

    def take_fin(s, h):
        down_copy(s, h).wait_recv()
        here = piece(fin, s, h)

        @pl.when(center & has_down)
        def _():
            here[...] = (piece(inc, s, h)[...].astype(F32) + here[...].astype(F32)).astype(BF16)

        @pl.when(center & outer)
        def _():
            here[...] = (piece(own, s, h)[...].astype(F32) + here[...].astype(F32)).astype(BF16)

        @pl.when(has_down)
        def _():
            down_copy(s, h).start()

    def reduce_step(z):
        for h in range(SUB):
            take_in(z - LAG_IN, h)

        s_mid = z - LAG_FIN

        @pl.when(center & has_down & (s_mid >= 0) & (s_mid < chunks))
        def _():
            for h in range(SUB - 1):
                take_fin(s_mid, h)

        s_fin = z - LAG_OUT

        @pl.when((s_fin >= 0) & (s_fin < chunks) & (outer | inner))
        def _():
            for h in range(SUB):
                take_fin(s_fin, h)
            emit(s_fin)

    def reduce_rest(z):
        s_mid = z - LAG_FIN - 1

        @pl.when(center & has_down & (s_mid >= 0) & (s_mid < chunks))
        def _():
            take_fin(s_mid, SUB - 1)
            emit(s_mid)

    def pair_copy(j):
        return remote(tbuf.at[(3 - j) % 2], pin.at[j], p_send.at[j], p_recv.at[j], to_p)

    def peer_copy(j):
        return remote(pin.at[j], rsin.at[j - 1], s_send.at[j], s_recv.at[j], {"fs": flip(f, j)})

    def term(owner, c):
        cols = pl.ds(pl.multiple_of(c * cw, cw), cw)
        block = gcat[:, owner].reshape(rows, 2 * ff)
        right = gall[c, pl.ds(0, turn)].reshape(2 * ff, cw)
        return jnp.dot(block, right, preferred_element_type=F32).astype(BF16), cols

    def turn_weights(c, carry):
        here = pl.ds(pl.multiple_of(c * cw, cw), cw)
        gall[c, pl.ds(0, turn)] = wcat[here, :].T.reshape(turn, ranks, rk, cw)
        return carry

    def exit_step(i):
        j = 3 - i // 2

        @pl.when((i >= 0) & (i < 8) & (i % 2 == 0))
        def _():
            @pl.when(j < 2)
            def _():
                pair_copy(j + 2).wait_send()

            def one(i, carry):
                for n in range(UNROLL):
                    value, cols = term(flip(f, j) * 2 + other, i * UNROLL + n)
                    tbuf[(3 - j) % 2, :, cols] = value
                return carry

            lax.fori_loop(0, parts // UNROLL, one, 0)
            pair_copy(j).start()

        @pl.when((i >= 0) & (i < 8) & (i % 2 == 1))
        def _():
            pair_copy(j).wait_recv()

            def one(i, carry):
                for n in range(UNROLL):
                    c = i * UNROLL + n
                    value, cols = term(flip(f, j) * 2 + t, c)
                    total = value.astype(F32) + pin[j, :, cols].astype(F32)
                    gh[c, :, pl.ds(0, cw)] = total
                    pin[j, :, cols] = total.astype(BF16)
                return carry

            lax.fori_loop(0, parts // UNROLL, one, 0)

            @pl.when(j > 0)
            def _():
                peer_copy(j).start()

    def vec_copy(n):
        dev = (to_p, to_a, to_b)[n]
        return remote(gv.at[n], gr.at[n], v_send.at[n], v_recv.at[n], dev)

    def rep_copy(i, incoming=False):
        at = (r - i + reps) % reps if incoming else r
        return remote(grep.at[at], grep.at[at], w_send.at[i], w_recv.at[i], {"rep": (r + i) % reps})

    def reload(k):
        return pltpu.make_async_copy(g_hbm.at[k], tbuf.at[0, pl.ds(k * rk, rk)], lsem.at[3 + k])

    def finish():
        for k in range(parts):
            reload(k).wait()
        for j in (3, 2, 1):
            peer_copy(j).wait_recv()
        gv[0] = jnp.zeros_like(gv[0])

        def one(k, carry):
            here = pl.ds(pl.multiple_of(k * rk, rk), rk)
            grads = jnp.concatenate([gh[c, here, pl.ds(0, cw)] for c in range(parts)], axis=1)
            for j in (2, 1, 0):
                grads = grads + rsin[j, here, :].astype(F32)
            floats = xbuf[k].astype(F32)
            inverse = lax.rsqrt(jnp.mean(floats * floats, axis=-1, keepdims=True) + norm_eps)
            unit = floats * inverse
            gv[0] = gv[0] + jnp.sum(grads * unit, axis=0, keepdims=True)
            scaled = grads * gain_ref[...]
            shift = inverse * jnp.mean(scaled * unit, axis=-1, keepdims=True)
            cot = tbuf[0, here, :].astype(F32)
            xbuf[k] = (cot + inverse * scaled - unit * shift).astype(BF16)
            return carry

        lax.fori_loop(0, parts, one, 0)
        pltpu.make_async_copy(xbuf, gi_out, lsem.at[0]).start()
        vec_copy(0).start()

    def drain(ph):
        places = (me, me, me, pos(1, t), pos(2, t), pos(1, t), pos(2, t), pos(3, t), pos(3, t))
        for kind, p in enumerate(places):
            part = {3: 2, 4: 1, 7: 1, 8: 2}.get(kind, 0)
            if ph == 0:
                size = rk // 2 if part else rk
                ref = nall.at[:, p, pl.ds(max(part - 1, 0) * size, size)]
            else:
                size = parts // 2 if part else parts
                ref = gall.at[:, pl.ds(max(part - 1, 0) * size, size), p]
            remote(ref, ref, ssem.at[kind, ph], rsem.at[kind, 0], to_p).wait_send()

    def gain_store():
        return pltpu.make_async_copy(gv.at[0], gg_out, lsem.at[1])

    def gain_total():
        for i in range(1, reps):
            rep_copy(i, True).wait_recv()
        total = grep[0]
        for i in range(1, reps):
            total = total + grep[i]
        for n in range(3):
            vec_copy(n).wait_send()
        gv[0] = total
        gain_store().start()

    def tick(q, carry):
        for ph in (0, 1):
            k = q - ph * parts

            @pl.when((k >= 0) & (k < parts))
            def _():
                copy(ph, k, 0, True).wait_recv()
                copy(ph, k, 3).start()
                copy(ph, k, 5).start()
                copy(ph, k, 1, True).wait_recv()
                copy(ph, k, 4).start()
                copy(ph, k, 6).start()

        for ph in (0, 1):
            k = q + AHEAD - ph * parts

            @pl.when((k >= 0) & (k < parts))
            def _():
                if ph == 0:
                    normalise(k)
                issue(ph, k)

        @pl.when(q == 1)
        def _():
            for c in local[1:3] + local[3 + parts:]:
                c.wait()

            def clear(k, carry):
                gh[k] = jnp.zeros_like(gh[k])
                return carry

            lax.fori_loop(0, parts, clear, 0)

        @pl.when((q >= 2) & (q < parts + 2))
        def _():
            dwt[q - 2] = own[2 * parts + q - 2].T

        late = q - 2 - parts

        @pl.when((late >= 0) & (late < parts - 1))
        def _():
            accumulate(late)

        z = q - parts - 1
        reduce_rest(z)

        for ph in (0, 1):
            k = q - 1 - ph * parts

            @pl.when((k >= 0) & (k < parts))
            def _():
                copy(ph, k, 3, True).wait_recv()
                copy(ph, k, 8).start()
                copy(ph, k, 4, True).wait_recv()
                copy(ph, k, 7).start()
                for kind in (2, 5, 6, 7, 8):
                    copy(ph, k, kind, True).wait_recv()
                if ph == 0:
                    forward(k)
                else:
                    grad_chunk(k)

        @pl.when((z >= 0) & (z < parts))
        def _():
            send_own(z)

        @pl.when((z >= parts) & (z < 2 * parts))
        def _():
            weight_pair(z - parts)
            send_own(2 * z - parts)
            send_own(2 * z - parts + 1)

        reduce_step(z)

        @pl.when(q == 2 * parts)
        def _():
            accumulate(parts - 1)
            lax.fori_loop(0, parts, elementwise, 0)

        @pl.when(q == EXIT_TICK - 1)
        def _():
            drain(0)
            drain(1)
            lax.fori_loop(0, parts, turn_weights, 0)

        @pl.when(q == EXIT_TICK + 8)
        def _():
            for j in (1, 0):
                pair_copy(j).wait_send()
            for k in range(parts):
                reload(k).start()

        exit_step(q - EXIT_TICK)

        @pl.when(q == FINISH)
        def _():
            finish()

        for n in (0, 1, 2):
            @pl.when(q == FINISH + 1 + n)
            def _():
                vec_copy(n).wait_recv()
                gv[n + 1] = gv[n] + gr[n]
                if n < 2:
                    vec_copy(n + 1).start()
                else:
                    grep[r] = gv[3]
                    for i in range(1, reps):
                        rep_copy(i).start()

        @pl.when(q == ticks - 1)
        def _():
            gain_total()

        return carry

    lax.fori_loop(0, ticks, tick, 0)

    remote(own, inc, up_send.at[0], in_recv.at[0, 0], up).wait_send()

    @pl.when(has_down)
    def _():
        remote(fin, fin, down_send.at[0], fin_recv.at[0, 0], down).wait_send()

    for j in (3, 2, 1):
        peer_copy(j).wait_send()
    for i in range(1, reps):
        rep_copy(i).wait_send()
    for s in (parts - 2, parts - 1):
        down_store(s).wait()
    for s in (chunks - 2, chunks - 1):
        gate_store(s, up_out).wait()
    pltpu.make_async_copy(xbuf, gi_out, lsem.at[0]).wait()
    gain_store().wait()


def widen_kernel(factor, *refs):
    arrays, rest = refs[:3], refs[3:5]
    outs, rest_outs = refs[5:8], refs[8:10]
    taken, given, held = refs[10:13], refs[13:16], refs[16:18]
    isem, osem, rsem, wsem = refs[18:]

    def rows(a, i):
        size = arrays[a].shape[0] // PIECES
        return pl.ds(i * size, size)

    def take(a, i):
        return pltpu.make_async_copy(arrays[a].at[rows(a, i)], taken[a].at[rows(a, i)], isem.at[a, i])

    def give(a, i):
        return pltpu.make_async_copy(given[a].at[rows(a, i)], outs[a].at[rows(a, i)], osem.at[a, i])

    order = [(a, i) for a in range(3) for i in range(PIECES)]
    for a, i in order:
        take(a, i).start()
    carried = [pltpu.make_async_copy(rest[n], held[n], rsem.at[n]) for n in range(2)]
    passed = [pltpu.make_async_copy(held[n], rest_outs[n], wsem.at[n]) for n in range(2)]
    for c in carried:
        c.start()
    for a, i in order:
        take(a, i).wait()
        scale = 0.5 * factor if a == 0 else factor
        given[a][rows(a, i), :] = taken[a][rows(a, i), :].astype(F32) * scale
        give(a, i).start()
    for n in range(2):
        carried[n].wait()
        passed[n].start()
    for a, i in order:
        give(a, i).wait()
    for c in passed:
        c.wait()


def shards(tokens_in, norm_gain, gate_weight, up_weight, down_weight, out_grad):
    rows, d = tokens_in.shape
    ff = gate_weight.shape[1]
    reps = lax.axis_size("rep")
    ranks = lax.axis_size("fs") * lax.axis_size("tp")
    factor = float(rows * reps * ranks) ** (-0.5)
    rk, cw = rows // PARTS, d // PARTS
    vmem, anywhere = pl.BlockSpec(memory_space=pltpu.VMEM), pl.BlockSpec(memory_space=pl.ANY)
    dma = pltpu.SemaphoreType.DMA
    chunks = 3 * PARTS
    shape = lambda *s: jax.ShapeDtypeStruct(s, F32)
    half = lambda *s: jax.ShapeDtypeStruct(s, BF16)
    narrow = lambda *s: pltpu.VMEM(s, BF16)
    wide = lambda *s: pltpu.VMEM(s, F32)
    grad_in, grad_gain, grad_down, grad_gate, grad_up = pl.pallas_call(
        lambda *refs: fused_kernel(reps, *refs),
        out_shape=[
            half(PARTS, rk, d), shape(1, d), half(ff, d), half(d, ff), half(d, ff),
        ],
        in_specs=[anywhere, anywhere, vmem, anywhere, anywhere, anywhere],
        out_specs=[anywhere] * 5,
        scratch_shapes=[
            narrow(PARTS, ranks, rk, d), narrow(PARTS, PARTS, ranks, rk, cw),
            narrow(d, 2 * ff), narrow(PARTS, cw, ff),
            wide(PARTS, ranks * rk, 2 * ff), wide(PARTS, ranks * rk, ff),
            narrow(2 * ff, PARTS * ranks * rk), narrow(PARTS, ranks, rk, 2 * ff),
            narrow(chunks, ff, cw), narrow(chunks, ff, cw), narrow(chunks, ff, cw),
            narrow(2, rows, d), narrow(4, rows, d), narrow(3, rows, d), narrow(PARTS, rk, d),
            narrow(2, cw, ff), wide(4, 1, d), wide(3, 1, d), wide(reps, 1, d),
            dma((9, 2)), dma((9, PARTS)), dma((3 + 2 * PARTS,)),
            dma((1,)), dma((chunks, SUB)), dma((1,)), dma((chunks, SUB)),
            dma((4,)), dma((4,)), dma((4,)), dma((4,)), dma((3,)), dma((3,)), dma((reps,)), dma((reps,)), dma((4,)),
        ],
        compiler_params=pltpu.CompilerParams(
            collective_id=0, has_side_effects=True, vmem_limit_bytes=63 * 2**20
        ),
        name="fused_backward",
    )(
        tokens_in.reshape(PARTS, rk, d), out_grad.reshape(PARTS, rk, d), norm_gain.reshape(1, d),
        gate_weight, up_weight, down_weight,
    )
    arrays = (grad_down, grad_gate, grad_up)
    outs = [shape(*a.shape) for a in arrays]
    grad_down, grad_gate, grad_up, grad_in, grad_gain = pl.pallas_call(
        lambda *refs: widen_kernel(factor, *refs),
        out_shape=outs + [half(rows, d), shape(1, d)],
        in_specs=[anywhere] * 5,
        out_specs=[anywhere] * 5,
        scratch_shapes=[narrow(*a.shape) for a in arrays] + [wide(*a.shape) for a in arrays] + [
            narrow(rows, d), wide(1, d), dma((3, PIECES)), dma((3, PIECES)), dma((2,)), dma((2,)),
        ],
        compiler_params=pltpu.CompilerParams(vmem_limit_bytes=63 * 2**20),
        name="widen",
    )(grad_down, grad_gate, grad_up, grad_in.reshape(rows, d), grad_gain)
    return (grad_in, grad_gain.reshape(d), grad_gate, grad_up, grad_down)


def solution(mesh):
    spread = ("fs", "tp")
    in_specs = (
        P(("rep", "fs", "tp"), None), P(), P(None, spread), P(None, spread), P(spread, None),
        P(("rep", "fs", "tp"), None),
    )
    out_specs = (
        P(("rep", "fs", "tp"), None), P(), P(None, spread), P(None, spread), P(spread, None),
    )
    return jax.shard_map(shards, mesh=mesh, in_specs=in_specs, out_specs=out_specs, check_vma=False)
```

```python
import jax
import jax.numpy as jnp
from jax import lax
from jax.experimental import pallas as pl
from jax.experimental.pallas import tpu as pltpu
from jax.sharding import PartitionSpec as P

norm_eps = 1e-06
MESH = pl.DeviceIdType.MESH
F32, BF16 = jnp.float32, jnp.bfloat16
NT = (((1,), (1,)), ((), ()))
PARTS = 8
AHEAD = 2
PIECES = 2
SUB = 2
LAG_IN = 1
LAG_FIN = 2
LAG_OUT = 6
EXIT_TICK = 2 * PARTS + 2
UNROLL = 8
FINISH = 31


def flip(f, j):
    return (f % 2 + j % 2) % 2 + 2 * ((f // 2 + j // 2) % 2)


def remote(src, dst, send, recv, dev):
    return pltpu.make_async_remote_copy(
        src_ref=src, dst_ref=dst, send_sem=send, recv_sem=recv, device_id=dev, device_id_type=MESH
    )


def fused_kernel(
    reps,
    x_hbm, g_hbm, gain_ref, gw_hbm, uw_hbm, dw_hbm,
    gi_out, gg_out, down_out, gate_out, up_out,
    nall, gall, wcat, dwt, act, gh, tcat, gcat, own, inc, fin,
    tbuf, pin, rsin, xbuf, stage_g, gv, gr, grep,
    ssem, rsem, lsem, up_send, in_recv, down_send, fin_recv,
    p_send, p_recv, s_send, s_recv, v_send, v_recv, w_send, w_recv, osem,
):
    f, t, r = lax.axis_index("fs"), lax.axis_index("tp"), lax.axis_index("rep")
    other = 1 - t
    parts, rk, d = xbuf.shape
    rows = parts * rk
    ff = dwt.shape[2]
    cw = d // parts
    ranks = gcat.shape[1]
    toks = ranks * rk
    chunks = 3 * parts
    sub = ff // SUB
    ticks = parts + 1 + chunks + LAG_OUT
    turn = 2 * ff // toks

    middle = reps // 2
    sign = 1 - 2 * (r // middle)
    up, down = {"rep": r + sign}, {"rep": (r - sign + reps) % reps}
    right = r // middle
    depth = (1 - right) * (middle - 1 - r) + right * (r - middle)
    center, outer = depth == 0, depth == middle - 1
    inner, has_down = depth > 0, depth < middle - 1
    to_a, to_b, to_p = {"fs": flip(f, 1)}, {"fs": flip(f, 2)}, {"tp": other}

    barrier = pltpu.get_barrier_semaphore()
    for dev in (to_a, to_b, {"fs": flip(f, 3)}, to_p):
        pl.semaphore_signal(barrier, inc=1, device_id=dev, device_id_type=MESH)
    for i in range(1, reps):
        pl.semaphore_signal(barrier, inc=1, device_id={"rep": (r + i) % reps}, device_id_type=MESH)

    def pos(j, core):
        return flip(f, j) * 2 + core

    me = pos(0, t)

    def loads():
        out = [pltpu.make_async_copy(x_hbm, xbuf, lsem.at[0])]
        out.append(pltpu.make_async_copy(gw_hbm, wcat.at[:, pl.ds(0, ff)], lsem.at[1]))
        out.append(pltpu.make_async_copy(uw_hbm, wcat.at[:, pl.ds(ff, ff)], lsem.at[2]))
        for c in range(parts):
            cols = pl.ds(c * cw, cw)
            out.append(pltpu.make_async_copy(g_hbm.at[:, :, cols], gall.at[c, :, me], lsem.at[3 + c]))
        for c in range(parts):
            cols = pl.ds(c * cw, cw)
            out.append(pltpu.make_async_copy(dw_hbm.at[:, cols], own.at[2 * parts + c], lsem.at[3 + parts]))
        return out

    local = loads()
    for c in local:
        c.start()

    def slot(ph, k, p, part=0):
        if ph == 0:
            ref = nall.at[k, p]
            size = rk // 2
        else:
            ref = gall.at[k, :, p]
            size = parts // 2
        if part == 0:
            return ref
        return ref.at[pl.ds((part - 1) * size, size)]

    def copy(ph, k, kind, incoming=False):
        sems = (ssem.at[kind, ph], rsem.at[kind, k])
        core = other if incoming else t
        if kind == 0:
            ref, dev = slot(ph, k, pos(1, t) if incoming else me), to_a
        elif kind == 1:
            ref, dev = slot(ph, k, pos(2, t) if incoming else me), to_b
        elif kind == 2:
            ref, dev = slot(ph, k, pos(0, core)), to_p
        elif kind == 3:
            ref, dev = slot(ph, k, pos(3, t) if incoming else pos(1, t), 2), to_b
        elif kind == 4:
            ref, dev = slot(ph, k, pos(3, t) if incoming else pos(2, t), 1), to_a
        elif kind == 5:
            ref, dev = slot(ph, k, pos(1, core)), to_p
        elif kind == 6:
            ref, dev = slot(ph, k, pos(2, core)), to_p
        else:
            ref, dev = slot(ph, k, pos(3, core), kind - 6), to_p
        return remote(ref, ref, *sems, dev)

    def normalise(k):
        floats = xbuf[k].astype(F32)
        inverse = lax.rsqrt(jnp.mean(floats * floats, axis=-1, keepdims=True) + norm_eps)
        nall[k, me] = (floats * inverse * gain_ref[...]).astype(BF16)

    def issue(ph, k):
        for kind in (0, 1, 2):
            copy(ph, k, kind).start()

    local[0].wait()
    for k in range(AHEAD):
        normalise(k)
    pl.semaphore_wait(barrier, 3 + reps)
    for k in range(AHEAD):
        issue(0, k)
    for c in local[3:3 + parts]:
        c.wait()

    def forward(k):
        block = nall[k].reshape(toks, d)
        pre = jnp.dot(block, wcat[...], preferred_element_type=F32)
        gate_pre, up_pre = pre[:, :ff], pre[:, ff:]
        sigma = jax.nn.sigmoid(gate_pre)
        active = gate_pre * sigma
        act[k, :, pl.ds(0, ff)] = up_pre * sigma * (1.0 + gate_pre * (1.0 - sigma))
        act[k, :, pl.ds(ff, ff)] = active
        cols = pl.ds(pl.multiple_of(k * toks, toks), toks)
        tcat[pl.ds(0, ff), cols] = (active * up_pre).T.astype(BF16)

    def grad_chunk(c):
        whole = gall[c].reshape(parts * toks, cw)
        own[c] = jnp.dot(tcat[pl.ds(0, ff), :], whole, preferred_element_type=F32).astype(BF16)

    def accumulate(c):
        def one(i, carry):
            for n in range(UNROLL):
                k = i * UNROLL + n
                block = gall[c, k].reshape(toks, cw)
                gh[k] = gh[k] + jnp.dot(block, dwt[c], preferred_element_type=F32)
            return carry

        lax.fori_loop(0, parts // UNROLL, one, 0)

    def elementwise(k, carry):
        half = 0.5 * gh[k]
        ggp = half * act[k, :, pl.ds(0, ff)]
        gup = half * act[k, :, pl.ds(ff, ff)]
        cols = pl.ds(pl.multiple_of(k * toks, toks), toks)
        gcat[k, :, :, pl.ds(0, ff)] = ggp.astype(BF16).reshape(ranks, rk, ff)
        gcat[k, :, :, pl.ds(ff, ff)] = gup.astype(BF16).reshape(ranks, rk, ff)
        tcat[pl.ds(0, ff), cols] = ggp.T.astype(BF16)
        tcat[pl.ds(ff, ff), cols] = gup.T.astype(BF16)
        return carry

    def weight_pair(c):
        cols = pl.ds(pl.multiple_of(c * cw, cw), cw)
        whole = nall[:, :, :, cols].reshape(parts * toks, cw)
        both = jnp.dot(tcat[...], whole, preferred_element_type=F32).astype(BF16)
        own[parts + 2 * c] = both[:ff]
        own[parts + 2 * c + 1] = both[ff:]

    def piece(ref, s, h):
        return ref.at[s, pl.ds(h * sub, sub)]

    def up_copy(s, h, src, dst, recv):
        return remote(piece(src, s, h), piece(dst, s, h), up_send.at[0], recv.at[s, h], up)

    def down_copy(s, h):
        return remote(piece(fin, s, h), piece(fin, s, h), down_send.at[0], fin_recv.at[s, h], down)

    def down_store(s):
        cols = pl.ds(pl.multiple_of(s * cw, cw), cw)
        return pltpu.make_async_copy(fin.at[s], down_out.at[:, cols], osem.at[s % 2])

    def gate_store(s, out):
        here = pl.ds(pl.multiple_of(((s - parts) // 2) * cw, cw), cw)
        return pltpu.make_async_copy(stage_g.at[s % 2], out.at[here], osem.at[2 + s % 2])

    def emit(s):
        @pl.when(s < parts)
        def _():
            @pl.when(s >= 2)
            def _():
                down_store(s - 2).wait()

            down_store(s).start()

        @pl.when(s >= parts)
        def _():
            @pl.when(s >= parts + 2)
            def _():
                gate_store(s - 2, gate_out).wait()

            stage_g[s % 2] = fin[s].T

            @pl.when(s % 2 == 0)
            def _():
                gate_store(s, gate_out).start()

            @pl.when(s % 2 == 1)
            def _():
                gate_store(s, up_out).start()

    def send_own(s):
        @pl.when(outer)
        def _():
            for h in range(SUB):
                @pl.when(center)
                def _():
                    up_copy(s, h, own, fin, fin_recv).start()

                @pl.when(inner)
                def _():
                    up_copy(s, h, own, inc, in_recv).start()

    def take_in(s, h):
        @pl.when(has_down & (s >= 0) & (s < chunks))
        def _():
            up_copy(s, h, inc, inc, in_recv).wait_recv()
            here = piece(inc, s, h)
            here[...] = (piece(own, s, h)[...].astype(F32) + here[...].astype(F32)).astype(BF16)

            @pl.when(center)
            def _():
                up_copy(s, h, inc, fin, fin_recv).start()

            @pl.when(inner)
            def _():
                up_copy(s, h, inc, inc, in_recv).start()

    def take_fin(s, h):
        down_copy(s, h).wait_recv()
        here = piece(fin, s, h)

        @pl.when(center & has_down)
        def _():
            here[...] = (piece(inc, s, h)[...].astype(F32) + here[...].astype(F32)).astype(BF16)

        @pl.when(center & outer)
        def _():
            here[...] = (piece(own, s, h)[...].astype(F32) + here[...].astype(F32)).astype(BF16)

        @pl.when(has_down)
        def _():
            down_copy(s, h).start()

    def reduce_step(z):
        for h in range(SUB):
            take_in(z - LAG_IN, h)

        s_mid = z - LAG_FIN

        @pl.when(center & has_down & (s_mid >= 0) & (s_mid < chunks))
        def _():
            for h in range(SUB - 1):
                take_fin(s_mid, h)

        s_fin = z - LAG_OUT

        @pl.when((s_fin >= 0) & (s_fin < chunks) & (outer | inner))
        def _():
            for h in range(SUB):
                take_fin(s_fin, h)
            emit(s_fin)

    def reduce_rest(z):
        s_mid = z - LAG_FIN - 1

        @pl.when(center & has_down & (s_mid >= 0) & (s_mid < chunks))
        def _():
            take_fin(s_mid, SUB - 1)
            emit(s_mid)

    def pair_copy(j):
        return remote(tbuf.at[(3 - j) % 2], pin.at[j], p_send.at[j], p_recv.at[j], to_p)

    def peer_copy(j):
        return remote(pin.at[j], rsin.at[j - 1], s_send.at[j], s_recv.at[j], {"fs": flip(f, j)})

    def term(owner, c):
        cols = pl.ds(pl.multiple_of(c * cw, cw), cw)
        block = gcat[:, owner].reshape(rows, 2 * ff)
        right = gall[c, pl.ds(0, turn)].reshape(2 * ff, cw)
        return jnp.dot(block, right, preferred_element_type=F32).astype(BF16), cols

    def turn_weights(c, carry):
        here = pl.ds(pl.multiple_of(c * cw, cw), cw)
        gall[c, pl.ds(0, turn)] = wcat[here, :].T.reshape(turn, ranks, rk, cw)
        return carry

    def exit_step(i):
        j = 3 - i // 2

        @pl.when((i >= 0) & (i < 8) & (i % 2 == 0))
        def _():
            @pl.when(j < 2)
            def _():
                pair_copy(j + 2).wait_send()

            def one(i, carry):
                for n in range(UNROLL):
                    value, cols = term(flip(f, j) * 2 + other, i * UNROLL + n)
                    tbuf[(3 - j) % 2, :, cols] = value
                return carry

            lax.fori_loop(0, parts // UNROLL, one, 0)
            pair_copy(j).start()

        @pl.when((i >= 0) & (i < 8) & (i % 2 == 1))
        def _():
            pair_copy(j).wait_recv()

            def one(i, carry):
                for n in range(UNROLL):
                    c = i * UNROLL + n
                    value, cols = term(flip(f, j) * 2 + t, c)
                    total = value.astype(F32) + pin[j, :, cols].astype(F32)
                    gh[c, :, pl.ds(0, cw)] = total
                    pin[j, :, cols] = total.astype(BF16)
                return carry

            lax.fori_loop(0, parts // UNROLL, one, 0)

            @pl.when(j > 0)
            def _():
                peer_copy(j).start()

    def vec_copy(n):
        dev = (to_p, to_a, to_b)[n]
        return remote(gv.at[n], gr.at[n], v_send.at[n], v_recv.at[n], dev)

    def rep_copy(i, incoming=False):
        at = (r - i + reps) % reps if incoming else r
        return remote(grep.at[at], grep.at[at], w_send.at[i], w_recv.at[i], {"rep": (r + i) % reps})

    def reload(k):
        return pltpu.make_async_copy(g_hbm.at[k], tbuf.at[0, pl.ds(k * rk, rk)], lsem.at[3 + k])

    def finish():
        for k in range(parts):
            reload(k).wait()
        for j in (3, 2, 1):
            peer_copy(j).wait_recv()
        gv[0] = jnp.zeros_like(gv[0])

        def one(k, carry):
            here = pl.ds(pl.multiple_of(k * rk, rk), rk)
            grads = jnp.concatenate([gh[c, here, pl.ds(0, cw)] for c in range(parts)], axis=1)
            for j in (2, 1, 0):
                grads = grads + rsin[j, here, :].astype(F32)
            floats = xbuf[k].astype(F32)
            inverse = lax.rsqrt(jnp.mean(floats * floats, axis=-1, keepdims=True) + norm_eps)
            unit = floats * inverse
            gv[0] = gv[0] + jnp.sum(grads * unit, axis=0, keepdims=True)
            scaled = grads * gain_ref[...]
            shift = inverse * jnp.mean(scaled * unit, axis=-1, keepdims=True)
            cot = tbuf[0, here, :].astype(F32)
            xbuf[k] = (cot + inverse * scaled - unit * shift).astype(BF16)
            return carry

        lax.fori_loop(0, parts, one, 0)
        pltpu.make_async_copy(xbuf, gi_out, lsem.at[0]).start()
        vec_copy(0).start()

    def drain(ph):
        places = (me, me, me, pos(1, t), pos(2, t), pos(1, t), pos(2, t), pos(3, t), pos(3, t))
        for kind, p in enumerate(places):
            part = {3: 2, 4: 1, 7: 1, 8: 2}.get(kind, 0)
            if ph == 0:
                size = rk // 2 if part else rk
                ref = nall.at[:, p, pl.ds(max(part - 1, 0) * size, size)]
            else:
                size = parts // 2 if part else parts
                ref = gall.at[:, pl.ds(max(part - 1, 0) * size, size), p]
            remote(ref, ref, ssem.at[kind, ph], rsem.at[kind, 0], to_p).wait_send()

    def gain_store():
        return pltpu.make_async_copy(gv.at[0], gg_out, lsem.at[1])

    def gain_total():
        for i in range(1, reps):
            rep_copy(i, True).wait_recv()
        total = grep[0]
        for i in range(1, reps):
            total = total + grep[i]
        for n in range(3):
            vec_copy(n).wait_send()
        gv[0] = total
        gain_store().start()

    def tick(q, carry):
        for ph in (0, 1):
            k = q - ph * parts

            @pl.when((k >= 0) & (k < parts))
            def _():
                copy(ph, k, 0, True).wait_recv()
                copy(ph, k, 3).start()
                copy(ph, k, 5).start()
                copy(ph, k, 1, True).wait_recv()
                copy(ph, k, 4).start()
                copy(ph, k, 6).start()

        for ph in (0, 1):
            k = q + AHEAD - ph * parts

            @pl.when((k >= 0) & (k < parts))
            def _():
                if ph == 0:
                    normalise(k)
                issue(ph, k)

        @pl.when(q == 1)
        def _():
            for c in local[1:3]:
                c.wait()
            raw = own.at[pl.ds(2 * parts, parts)]
            pltpu.make_async_copy(raw, raw, lsem.at[3 + parts]).wait()

            def clear(k, carry):
                gh[k] = jnp.zeros_like(gh[k])
                return carry

            lax.fori_loop(0, parts, clear, 0)

        @pl.when((q >= 2) & (q < parts + 2))
        def _():
            dwt[q - 2] = own[2 * parts + q - 2].T

        late = q - 2 - parts

        @pl.when((late >= 0) & (late < parts - 1))
        def _():
            accumulate(late)

        z = q - parts - 1
        reduce_rest(z)

        for ph in (0, 1):
            k = q - 1 - ph * parts

            @pl.when((k >= 0) & (k < parts))
            def _():
                copy(ph, k, 3, True).wait_recv()
                copy(ph, k, 8).start()
                copy(ph, k, 4, True).wait_recv()
                copy(ph, k, 7).start()
                for kind in (2, 5, 6, 7, 8):
                    copy(ph, k, kind, True).wait_recv()
                if ph == 0:
                    forward(k)
                else:
                    grad_chunk(k)

        @pl.when((z >= 0) & (z < parts))
        def _():
            send_own(z)

        @pl.when((z >= parts) & (z < 2 * parts))
        def _():
            weight_pair(z - parts)
            send_own(2 * z - parts)
            send_own(2 * z - parts + 1)

        reduce_step(z)

        @pl.when(q == 2 * parts)
        def _():
            accumulate(parts - 1)
            lax.fori_loop(0, parts, elementwise, 0)

        @pl.when(q == EXIT_TICK - 1)
        def _():
            drain(0)
            drain(1)
            lax.fori_loop(0, parts, turn_weights, 0)

        @pl.when(q == EXIT_TICK + 8)
        def _():
            for j in (1, 0):
                pair_copy(j).wait_send()
            for k in range(parts):
                reload(k).start()

        exit_step(q - EXIT_TICK)

        @pl.when(q == FINISH)
        def _():
            finish()

        for n in (0, 1, 2):
            @pl.when(q == FINISH + 1 + n)
            def _():
                vec_copy(n).wait_recv()
                gv[n + 1] = gv[n] + gr[n]
                if n < 2:
                    vec_copy(n + 1).start()
                else:
                    grep[r] = gv[3]
                    for i in range(1, reps):
                        rep_copy(i).start()

        @pl.when(q == ticks - 1)
        def _():
            gain_total()

        return carry

    lax.fori_loop(0, ticks, tick, 0)

    remote(own, inc, up_send.at[0], in_recv.at[0, 0], up).wait_send()

    @pl.when(has_down)
    def _():
        remote(fin, fin, down_send.at[0], fin_recv.at[0, 0], down).wait_send()

    for j in (3, 2, 1):
        peer_copy(j).wait_send()
    for i in range(1, reps):
        rep_copy(i).wait_send()
    for s in (parts - 2, parts - 1):
        down_store(s).wait()
    for s in (chunks - 2, chunks - 1):
        gate_store(s, up_out).wait()
    pltpu.make_async_copy(xbuf, gi_out, lsem.at[0]).wait()
    gain_store().wait()


def widen_kernel(factor, *refs):
    arrays, rest = refs[:3], refs[3:5]
    outs, rest_outs = refs[5:8], refs[8:10]
    taken, given, held = refs[10:13], refs[13:16], refs[16:18]
    isem, osem, rsem, wsem = refs[18:]

    def rows(a, i):
        size = arrays[a].shape[0] // PIECES
        return pl.ds(i * size, size)

    def take(a, i):
        return pltpu.make_async_copy(arrays[a].at[rows(a, i)], taken[a].at[rows(a, i)], isem.at[a, i])

    def give(a, i):
        return pltpu.make_async_copy(given[a].at[rows(a, i)], outs[a].at[rows(a, i)], osem.at[a, i])

    order = [(a, i) for a in range(3) for i in range(PIECES)]
    for a, i in order:
        take(a, i).start()
    carried = [pltpu.make_async_copy(rest[n], held[n], rsem.at[n]) for n in range(2)]
    passed = [pltpu.make_async_copy(held[n], rest_outs[n], wsem.at[n]) for n in range(2)]
    for c in carried:
        c.start()
    for a, i in order:
        take(a, i).wait()
        scale = 0.5 * factor if a == 0 else factor
        given[a][rows(a, i), :] = taken[a][rows(a, i), :].astype(F32) * scale
        give(a, i).start()
    for n in range(2):
        carried[n].wait()
        passed[n].start()
    for a, i in order:
        give(a, i).wait()
    for c in passed:
        c.wait()


def shards(tokens_in, norm_gain, gate_weight, up_weight, down_weight, out_grad):
    rows, d = tokens_in.shape
    ff = gate_weight.shape[1]
    reps = lax.axis_size("rep")
    ranks = lax.axis_size("fs") * lax.axis_size("tp")
    factor = float(rows * reps * ranks) ** (-0.5)
    rk, cw = rows // PARTS, d // PARTS
    vmem, anywhere = pl.BlockSpec(memory_space=pltpu.VMEM), pl.BlockSpec(memory_space=pl.ANY)
    dma = pltpu.SemaphoreType.DMA
    chunks = 3 * PARTS
    shape = lambda *s: jax.ShapeDtypeStruct(s, F32)
    half = lambda *s: jax.ShapeDtypeStruct(s, BF16)
    narrow = lambda *s: pltpu.VMEM(s, BF16)
    wide = lambda *s: pltpu.VMEM(s, F32)
    grad_in, grad_gain, grad_down, grad_gate, grad_up = pl.pallas_call(
        lambda *refs: fused_kernel(reps, *refs),
        out_shape=[
            half(PARTS, rk, d), shape(1, d), half(ff, d), half(d, ff), half(d, ff),
        ],
        in_specs=[anywhere, anywhere, vmem, anywhere, anywhere, anywhere],
        out_specs=[anywhere] * 5,
        scratch_shapes=[
            narrow(PARTS, ranks, rk, d), narrow(PARTS, PARTS, ranks, rk, cw),
            narrow(d, 2 * ff), narrow(PARTS, cw, ff),
            wide(PARTS, ranks * rk, 2 * ff), wide(PARTS, ranks * rk, ff),
            narrow(2 * ff, PARTS * ranks * rk), narrow(PARTS, ranks, rk, 2 * ff),
            narrow(chunks, ff, cw), narrow(chunks, ff, cw), narrow(chunks, ff, cw),
            narrow(2, rows, d), narrow(4, rows, d), narrow(3, rows, d), narrow(PARTS, rk, d),
            narrow(2, cw, ff), wide(4, 1, d), wide(3, 1, d), wide(reps, 1, d),
            dma((9, 2)), dma((9, PARTS)), dma((4 + PARTS,)),
            dma((1,)), dma((chunks, SUB)), dma((1,)), dma((chunks, SUB)),
            dma((4,)), dma((4,)), dma((4,)), dma((4,)), dma((3,)), dma((3,)), dma((reps,)), dma((reps,)), dma((4,)),
        ],
        compiler_params=pltpu.CompilerParams(
            collective_id=0, has_side_effects=True, vmem_limit_bytes=63 * 2**20
        ),
        name="fused_backward",
    )(
        tokens_in.reshape(PARTS, rk, d), out_grad.reshape(PARTS, rk, d), norm_gain.reshape(1, d),
        gate_weight, up_weight, down_weight,
    )
    arrays = (grad_down, grad_gate, grad_up)
    outs = [shape(*a.shape) for a in arrays]
    grad_down, grad_gate, grad_up, grad_in, grad_gain = pl.pallas_call(
        lambda *refs: widen_kernel(factor, *refs),
        out_shape=outs + [half(rows, d), shape(1, d)],
        in_specs=[anywhere] * 5,
        out_specs=[anywhere] * 5,
        scratch_shapes=[narrow(*a.shape) for a in arrays] + [wide(*a.shape) for a in arrays] + [
            narrow(rows, d), wide(1, d), dma((3, PIECES)), dma((3, PIECES)), dma((2,)), dma((2,)),
        ],
        compiler_params=pltpu.CompilerParams(vmem_limit_bytes=63 * 2**20),
        name="widen",
    )(grad_down, grad_gate, grad_up, grad_in.reshape(rows, d), grad_gain)
    return (grad_in, grad_gain.reshape(d), grad_gate, grad_up, grad_down)


def solution(mesh):
    spread = ("fs", "tp")
    in_specs = (
        P(("rep", "fs", "tp"), None), P(), P(None, spread), P(None, spread), P(spread, None),
        P(("rep", "fs", "tp"), None),
    )
    out_specs = (
        P(("rep", "fs", "tp"), None), P(), P(None, spread), P(None, spread), P(spread, None),
    )
    return jax.shard_map(shards, mesh=mesh, in_specs=in_specs, out_specs=out_specs, check_vma=False)
```
